32 devices in a mesh: grp: 2 (over x), ep: 8 (over z, y), tp: 2 (over core).
Axes of the slice: x: 2, y: 2, z: 4, core: 2. Of those that a mesh axis runs over, the one named last changes fastest.
Arguments:
- hidden_in: bfloat16 [256, 2048], P(('grp', 'ep', 'tp')), parts along dimension 0, may hold values from -6 to 6
- query_nope: bfloat16 [256, 16, 64], P(('grp', 'ep', 'tp')), parts along dimension 0, may hold values from -102 to 102
- query_rope: bfloat16 [256, 16, 32], P(('grp', 'ep', 'tp')), parts along dimension 0, may hold values from -6 to 6
- new_latent: bfloat16 [256, 256], P(('grp', 'ep', 'tp')), parts along dimension 0, may hold values from -6 to 6
- new_rope: bfloat16 [256, 32], P(('grp', 'ep', 'tp')), parts along dimension 0, may hold values from -6 to 6
- cache_latent: bfloat16 [256, 1024, 256], P(('grp', 'ep', 'tp')), parts along dimension 0, may hold values from -6 to 6
- cache_rope: bfloat16 [256, 1024, 32], P(('grp', 'ep', 'tp')), parts along dimension 0, may hold values from -6 to 6
- lengths: int32 [256], P(('grp', 'ep', 'tp')), parts along dimension 0, may hold values from 1 to 1024, as said below
- absorb_key: bfloat16 [256, 16, 64], replicated, may hold values from -0.75 to 0.75
- value_up: bfloat16 [256, 16, 128], replicated, may hold values from -0.375 to 0.375
- out_proj: bfloat16 [2048, 2048], P(None, ('ep', 'tp')), may hold values from -0.125 to 0.125
- gain_mix: bfloat16 [2048], replicated, may hold values from 0.099609375 to 1.8984375
- gain_ffn_in: bfloat16 [2048], replicated, may hold values from 0.099609375 to 1.8984375
- router: bfloat16 [2048, 16], replicated, may hold values from -0.125 to 0.125
- routes: int32 [256, 6], P(('grp', 'ep')), parts along dimension 0, may hold values from 0 to 15, all different within a row; in each aligned block of 16 rows (0 to 15, 16 to 31, ...) at most 12 rows name the same one
- expert_gate: bfloat16 [16, 2048, 256], P(('ep', 'tp')), may hold values from -0.125 to 0.125
- expert_up: bfloat16 [16, 2048, 256], P(('ep', 'tp')), may hold values from -0.125 to 0.125
- expert_down: bfloat16 [16, 256, 2048], P(('ep', 'tp')), may hold values from -0.375 to 0.375
- shared_gate: bfloat16 [2048, 256], replicated, may hold values from -0.125 to 0.125
- shared_up: bfloat16 [2048, 256], replicated, may hold values from -0.125 to 0.125
- shared_down: bfloat16 [256, 2048], replicated, may hold values from -0.375 to 0.375
- gain_ffn_out: bfloat16 [2048], replicated, may hold values from 0.099609375 to 1.8984375
Outputs:
- layer_out: bfloat16 [256, 2048], P(('grp', 'ep', 'tp')), parts along dimension 0
The draws below stay inside these ranges and needn't reach their ends.
There are 2 independent parts, one for each index of `grp`. The reference program is written for one: setup_inputs(seed, part) draws one part's arguments, and reference() takes and returns one part's arrays. A program takes and returns all parts, laid end to end along the dimension named above; an argument that names none is the same for every part. Nothing has to cross between parts.
Inputs may be any that keep to these rules, and one draw needn't show every extreme that they name: `lengths`: every sequence holds 1 to 1024 cached positions, and some sequence holds 1024. `routes`: each row names 6 different experts; in each aligned block of 16 rows (the rows of one index of ep) no expert is named by more than 12 rows, and in some block some expert is named by exactly 12 rows.
All inputs are finite; a program needn't handle non-finite values.
Results may differ from the reference program's by a relative error of at most 0.015.
Values may be sent and summed in bfloat16 or wider, within the bound.
A program may use at most 64 MiB of HBM per device.

```python
import math
import jax
import jax.numpy as jnp
import numpy as np
from jax import lax

D = 2048
HEADS = 16
NOPE = 64
ROPE = 32
VHEAD = 128
LAT = 256
FE = 256
FS = 256
TOPK = 6
CTX = 1024
SEQ_DEV = 8
NSEQ = 128
TOK_GROUP = 16
EXPERTS = 16
CAP = 12
N_EP = 8


def draw_query_nope(key, part):
    base_key = jax.random.fold_in(jax.random.fold_in(key, 23), 0)
    values = jnp.clip(jax.random.normal(base_key, (NSEQ, HEADS, NOPE), jnp.float32), -6.0, 6.0)
    return values.astype(jnp.bfloat16)


def draw_lengths(key, part):
    level_key, value_key, pick_key = jax.random.split(jax.random.fold_in(key, 11), 3)
    device_count = NSEQ // SEQ_DEV
    level_draw = jax.random.randint(level_key, (device_count,), 1, 5)
    length_limit = jnp.maximum(jnp.repeat(level_draw * level_draw * CTX // 16, SEQ_DEV), 1)
    raw_draw = jax.random.randint(value_key, (NSEQ,), 0, 1 << 20)
    drawn_lengths = 1 + raw_draw % length_limit
    chosen_row = jax.random.randint(pick_key, (), 0, NSEQ)
    drawn_lengths = jnp.where(jnp.arange(NSEQ) == chosen_row, CTX, drawn_lengths)
    return drawn_lengths.astype(jnp.int32)


def steps_of(stream_key, shape, pieces, low, high):
    def one(axis_at, shards_of):
        draws = jax.random.uniform(jax.random.fold_in(jax.random.fold_in(stream_key, 6), axis_at), (shards_of,), jnp.float32, low / len(pieces), high / len(pieces))
        return jnp.repeat(jnp.exp(draws), shape[axis_at] // shards_of).reshape((-1,) + (1,) * (len(shape) - axis_at - 1))

    gain = one(*pieces[0])
    for cut in pieces[1:]:
        gain = gain * one(*cut)
    return gain


def routed_block(own_key, own, number, rows, count, top, limit, slope):
    order = jax.random.permutation(own_key, count)
    crowded, usual = shares(count, rows * top, limit, slope, True), shares(count, rows * top, limit, slope, False)
    places = jnp.arange(count)

    def named(sizes, offset_by):
        used = int((sizes > 0).sum())
        fixed = max(1, used // 4)
        shifted = fixed + (places - fixed + offset_by * (used - fixed)) % max(1, count - fixed)
        return jnp.zeros((count,), jnp.int32).at[order[jnp.where(places < fixed, places, shifted)]].set(jnp.asarray(sizes, jnp.int32))

    sizes = jnp.where(number % 4 == 0, named(crowded, number // 4), named(usual, number - number // 4 - 1))
    mixed = jax.random.permutation(jax.random.fold_in(own, 3), count)
    giver, sink = mixed[0:count // 2 * 2:2], mixed[1:count // 2 * 2:2]
    margin = jnp.minimum(sizes[giver] - 1, limit - sizes[sink]) // 2
    margin = jnp.where((giver == order[0]) | (sink == order[0]) | (sizes[sink] == 0), 0, jnp.maximum(margin, 0))
    shifted = jax.random.randint(jax.random.fold_in(own, 4), (count // 2,), 0, 1 << 20) % (margin + 1)
    sizes = sizes.at[giver].add(-shifted).at[sink].add(shifted)
    items = jnp.searchsorted(jnp.cumsum(sizes), jnp.arange(rows * top), side="right").astype(jnp.int32)
    grid = items.reshape(top, rows).T
    grid = grid[jax.random.permutation(jax.random.fold_in(own, 1), rows)]
    offset_by = jax.random.randint(jax.random.fold_in(own, 2), (rows, 1), 0, top)
    return jnp.take_along_axis(grid, (jnp.arange(top)[None, :] + offset_by) % top, axis=1)


def shares(count, total, limit, lean, full):
    loads = [(1 << 20) // math.isqrt(rank ** lean) + 1 for rank in range(1, count + 1)]
    largest = limit if full else min(limit, max(-(-total // count), total * loads[0] // sum(loads)))
    least = 1 if total - largest >= count - 1 else 0
    counts, surplus = [largest] + [least] * (count - 1), total - largest - least * (count - 1)
    while surplus > 0:
        candidates = [i for i in range(1, count) if counts[i] < largest] or [i for i in range(1, count) if counts[i] < limit]
        whole, budget = sum([loads[i] for i in candidates]), surplus
        for i in candidates:
            addition = min(limit - counts[i], max(1, budget * loads[i] // whole), surplus)
            counts[i] = counts[i] + addition
            surplus = surplus - addition
    return np.array(counts)


def bell_draw(rng, shape, width, reach, pieces=(), kind=jnp.bfloat16):
    drawn = jax.random.normal(rng, shape, jnp.float32) * width
    if len(pieces) > 0:
        drawn = steps_of(rng, shape, pieces, -0.22, 0.18) * drawn
    return jnp.clip(drawn, min=-reach, max=reach).astype(kind)


def setup_inputs(seed: int = 0, part: int = 0) -> dict:
    key_of = jax.random.split(jax.random.key(seed), 23)
    own_keys = jax.random.split(jax.random.fold_in(key_of[22], part), 23)
    hidden_in = bell_draw(own_keys[0], (NSEQ, D), 1.0, 6.0, ((0, 16),))
    query_nope = draw_query_nope(jax.random.fold_in(jax.random.fold_in(key_of[22], part), 71), part)
    query_rope = bell_draw(own_keys[2], (NSEQ, HEADS, ROPE), 1.0, 6.0, ((0, 16),))
    new_latent = bell_draw(own_keys[3], (NSEQ, LAT), 1.0, 6.0, ((0, 16),))
    new_rope = bell_draw(own_keys[4], (NSEQ, ROPE), 1.0, 6.0, ((0, 16),))
    cache_latent = bell_draw(own_keys[5], (NSEQ, CTX, LAT), 1.0, 6.0, ((0, 16),))
    cache_rope = bell_draw(own_keys[6], (NSEQ, CTX, ROPE), 1.0, 6.0, ((0, 16),))
    lengths = draw_lengths(jax.random.fold_in(jax.random.fold_in(key_of[22], part), 71), part)
    absorb_key = bell_draw(key_of[8], (LAT, HEADS, NOPE), NOPE ** -0.5, 0.75)
    value_up = bell_draw(key_of[9], (LAT, HEADS, VHEAD), LAT ** -0.5, 0.375)
    out_proj = bell_draw(key_of[10], (HEADS * VHEAD, D), (HEADS * VHEAD) ** -0.5, 0.125, ((1, 16),))
    gain_mix = jnp.clip(1.0 + 0.18 * jax.random.normal(key_of[11], (D,), jnp.float32), 0.099609375, 1.8984375).astype(jnp.bfloat16)
    gain_ffn_in = jnp.clip(1.0 + 0.18 * jax.random.normal(key_of[12], (D,), jnp.float32), 0.099609375, 1.8984375).astype(jnp.bfloat16)
    router = bell_draw(key_of[13], (D, EXPERTS), D ** -0.5, 0.125)
    routes_keys = jax.random.split(jax.random.fold_in(own_keys[14], 1), NSEQ // TOK_GROUP)
    routes_turns = jax.random.permutation(jax.random.fold_in(own_keys[14], 3), NSEQ // TOK_GROUP)
    routes = jax.vmap(lambda own, number: routed_block(jax.random.fold_in(own_keys[14], 2), own, number, TOK_GROUP, EXPERTS, TOPK, CAP, 2))(routes_keys, routes_turns).reshape((NSEQ, TOPK))
    expert_gate = bell_draw(key_of[15], (EXPERTS, D, FE), D ** -0.5, 0.125, ((0, 16),))
    expert_up = bell_draw(key_of[16], (EXPERTS, D, FE), D ** -0.5, 0.125, ((0, 16),))
    expert_down = bell_draw(key_of[17], (EXPERTS, FE, D), FE ** -0.5, 0.375, ((0, 16),))
    shared_gate = bell_draw(key_of[18], (D, FS), D ** -0.5, 0.125)
    shared_up = bell_draw(key_of[19], (D, FS), D ** -0.5, 0.125)
    shared_down = bell_draw(key_of[20], (FS, D), FS ** -0.5, 0.375)
    gain_ffn_out = jnp.clip(1.0 + 0.18 * jax.random.normal(key_of[21], (D,), jnp.float32), 0.099609375, 1.8984375).astype(jnp.bfloat16)
    return dict(hidden_in=hidden_in, query_nope=query_nope, query_rope=query_rope, new_latent=new_latent, new_rope=new_rope, cache_latent=cache_latent, cache_rope=cache_rope, lengths=lengths, absorb_key=absorb_key, value_up=value_up, out_proj=out_proj, gain_mix=gain_mix, gain_ffn_in=gain_ffn_in, router=router, routes=routes, expert_gate=expert_gate, expert_up=expert_up, expert_down=expert_down, shared_gate=shared_gate, shared_up=shared_up, shared_down=shared_down, gain_ffn_out=gain_ffn_out)


rope_theta = 10000.0
norm_eps = 1e-06
routed_scale = 2.5
masked_score = -1e+30

def normalize(values):
    return values * lax.rsqrt(lax.optimization_barrier(jnp.mean(values * values, axis=-1, keepdims=True)) + norm_eps)

def rotate(values, positions):
    half_dim = values.shape[-1] // 2
    inverse = rope_theta ** (-jnp.arange(half_dim, dtype=jnp.float32) * 2.0 / values.shape[-1])
    angles = positions * inverse
    cosine = jnp.cos(angles)
    sine_table = jnp.sin(angles)
    first_half = values[..., :half_dim]
    second_half = values[..., half_dim:]
    return jnp.concatenate([first_half * cosine - second_half * sine_table, first_half * sine_table + second_half * cosine], axis=-1)

def swiglu(flat_rows, gate_w, up_w, down_w):
    gate_part = jnp.dot(flat_rows, gate_w, preferred_element_type=jnp.float32)
    up_part = jnp.dot(flat_rows, up_w, preferred_element_type=jnp.float32)
    inner_rows = (jax.nn.silu(gate_part) * up_part).astype(jnp.bfloat16)
    return jnp.dot(inner_rows, down_w, preferred_element_type=jnp.float32).astype(jnp.bfloat16)

def attend_group(group_args):
    query_latent, query_pe, latent_block, rope_block, latent_new, key_new, group_lengths = group_args
    score_scale = (NOPE + ROPE) ** (-0.5)
    cache_scores = (jnp.einsum('shc,skc->shk', query_latent.astype(jnp.float32), latent_block.astype(jnp.float32)) + jnp.einsum('shr,skr->shk', query_pe.astype(jnp.float32), rope_block.astype(jnp.float32))) * score_scale
    new_score = (jnp.einsum('shc,sc->sh', query_latent.astype(jnp.float32), latent_new.astype(jnp.float32)) + jnp.einsum('shr,sr->sh', query_pe.astype(jnp.float32), key_new.astype(jnp.float32))) * score_scale
    in_range = jnp.arange(CTX, dtype=jnp.int32)[None, None, :] < group_lengths[:, None, None]
    cache_scores = jnp.where(in_range, cache_scores, masked_score)
    row_max = jnp.maximum(lax.optimization_barrier(jnp.max(cache_scores, axis=-1)), new_score)
    cache_exp = jnp.exp(cache_scores - row_max[..., None])
    new_exp = jnp.exp(new_score - row_max)
    weight_total = lax.optimization_barrier(jnp.sum(cache_exp, axis=-1)) + new_exp
    cache_weights = lax.optimization_barrier(cache_exp.astype(jnp.bfloat16)).astype(jnp.float32)
    new_weight = lax.optimization_barrier(new_exp.astype(jnp.bfloat16)).astype(jnp.float32)
    weighted = jnp.einsum('shk,skc->shc', cache_weights, latent_block.astype(jnp.float32)) + new_weight[..., None] * latent_new.astype(jnp.float32)[:, None, :]
    return (weighted / weight_total[..., None]).astype(jnp.bfloat16)

def expert_apply(expert_args):
    flat_rows, gate_w, up_w, down_w = expert_args
    return swiglu(flat_rows, gate_w, up_w, down_w)

def reference(hidden_in, query_nope, query_rope, new_latent, new_rope, cache_latent, cache_rope, lengths, absorb_key, value_up, out_proj, gain_mix, gain_ffn_in, router, routes, expert_gate, expert_up, expert_down, shared_gate, shared_up, shared_down, gain_ffn_out):
    seq_count = hidden_in.shape[0]
    group_count = seq_count // SEQ_DEV
    positions = lengths.astype(jnp.float32)
    query_latent = jnp.einsum('shn,chn->shc', query_nope.astype(jnp.float32), absorb_key.astype(jnp.float32)).astype(jnp.bfloat16)
    query_pe = rotate(query_rope.astype(jnp.float32), positions[:, None, None]).astype(jnp.bfloat16)
    latent_new = normalize(new_latent.astype(jnp.float32)).astype(jnp.bfloat16)
    key_new = rotate(new_rope.astype(jnp.float32), positions[:, None]).astype(jnp.bfloat16)

    def grouped(values):
        return values.reshape((group_count, SEQ_DEV) + values.shape[1:])
    latent_out = lax.map(attend_group, (grouped(query_latent), grouped(query_pe), grouped(cache_latent), grouped(cache_rope), grouped(latent_new), grouped(key_new), grouped(lengths)))
    latent_out = latent_out.reshape(seq_count, HEADS, LAT)
    heads_out = jnp.einsum('shc,chv->shv', latent_out.astype(jnp.float32), value_up.astype(jnp.float32)).astype(jnp.bfloat16).reshape(seq_count, HEADS * VHEAD)
    mixed_rows = jnp.dot(heads_out, out_proj, preferred_element_type=jnp.float32).astype(jnp.bfloat16)
    after_mix = (hidden_in.astype(jnp.float32) + gain_mix.astype(jnp.float32) * normalize(mixed_rows.astype(jnp.float32))).astype(jnp.bfloat16)
    ffn_in = (normalize(after_mix.astype(jnp.float32)) * gain_ffn_in.astype(jnp.float32)).astype(jnp.bfloat16)
    affinity = jax.nn.sigmoid(jnp.dot(ffn_in, router, preferred_element_type=jnp.float32))
    chosen = jnp.take_along_axis(affinity, routes, axis=1)
    route_weights = chosen / lax.optimization_barrier(jnp.sum(chosen, axis=-1, keepdims=True)) * routed_scale
    pair_count = TOK_GROUP * TOPK
    expert_ids = routes.reshape(N_EP, pair_count)
    order_index = jnp.arange(pair_count, dtype=jnp.int32)
    same_expert = expert_ids[:, :, None] == expert_ids[:, None, :]
    earlier = order_index[None, :] < order_index[:, None]
    slot_number = lax.optimization_barrier(jnp.sum(jnp.logical_and(same_expert, earlier[None]), axis=2)).astype(jnp.int32)
    slot_number = slot_number.reshape(seq_count, TOPK)
    group_index = (jnp.arange(seq_count, dtype=jnp.int32) // TOK_GROUP)[:, None]
    slot_index = (routes * (N_EP * CAP) + group_index * CAP + slot_number).astype(jnp.int32)
    buffer = jnp.zeros((EXPERTS * N_EP * CAP, D), jnp.bfloat16)
    buffer = buffer.at[slot_index.reshape(-1)].set(jnp.repeat(ffn_in, TOPK, axis=0))
    outputs = lax.map(expert_apply, (buffer.reshape(EXPERTS, N_EP * CAP, D), expert_gate, expert_up, expert_down))
    picked = outputs.reshape(EXPERTS * N_EP * CAP, D)[slot_index]
    routed = lax.optimization_barrier(jnp.sum(picked.astype(jnp.float32) * route_weights[..., None], axis=1))
    shared = swiglu(ffn_in, shared_gate, shared_up, shared_down)
    combined = routed + shared.astype(jnp.float32)
    return (after_mix.astype(jnp.float32) + gain_ffn_out.astype(jnp.float32) * normalize(combined)).astype(jnp.bfloat16)
```

```python
import functools

import jax
import jax.numpy as jnp
from jax import lax
from jax.experimental import pallas as pl
from jax.experimental.pallas import tpu as pltpu
from jax.sharding import PartitionSpec as P

ABLK = 512


rope_theta = 10000.0
norm_eps = 1e-06
routed_scale = 2.5
masked_score = -1e30


def normalize(values):
    return values * lax.rsqrt(jnp.mean(values * values, axis=-1, keepdims=True) + norm_eps)


def rotate(values, positions):
    half_dim = values.shape[-1] // 2
    inverse = rope_theta ** (-jnp.arange(half_dim, dtype=jnp.float32) * 2.0 / values.shape[-1])
    angles = positions * inverse
    cosine = jnp.cos(angles)
    sine_table = jnp.sin(angles)
    first_half = values[..., :half_dim]
    second_half = values[..., half_dim:]
    return jnp.concatenate(
        [
            first_half * cosine - second_half * sine_table,
            first_half * sine_table + second_half * cosine,
        ],
        axis=-1,
    )


def swiglu(flat_rows, gate_w, up_w, down_w):
    gate_part = jnp.dot(flat_rows, gate_w, preferred_element_type=jnp.float32)
    up_part = jnp.dot(flat_rows, up_w, preferred_element_type=jnp.float32)
    inner_rows = (jax.nn.silu(gate_part) * up_part).astype(jnp.bfloat16)
    return jnp.dot(inner_rows, down_w, preferred_element_type=jnp.float32).astype(jnp.bfloat16)


def local_wide(
    hidden_in,
    query_nope,
    query_rope,
    new_latent,
    new_rope,
    cache_latent,
    cache_rope,
    lengths,
    absorb_key,
    value_up,
    out_proj,
    gain_mix,
    gain_ffn_in,
    router,
    routes,
    expert_gate,
    expert_up,
    expert_down,
    shared_gate,
    shared_up,
    shared_down,
    gain_ffn_out,
):
    seq_count = hidden_in.shape[0]
    positions = lengths.astype(jnp.float32)
    query_latent = jnp.einsum(
        "shn,chn->shc", query_nope, absorb_key, preferred_element_type=jnp.float32
    ).astype(jnp.bfloat16)
    query_pe = rotate(query_rope.astype(jnp.float32), positions[:, None, None]).astype(jnp.bfloat16)
    latent_new = normalize(new_latent.astype(jnp.float32)).astype(jnp.bfloat16)
    key_new = rotate(new_rope.astype(jnp.float32), positions[:, None]).astype(jnp.bfloat16)
    score_scale = (query_nope.shape[-1] + query_rope.shape[-1]) ** (-0.5)
    new_score = (
        jnp.einsum("shc,sc->sh", query_latent, latent_new, preferred_element_type=jnp.float32)
        + jnp.einsum("shr,sr->sh", query_pe, key_new, preferred_element_type=jnp.float32)
    ) * score_scale

    def attend_block(block_index, loop_state):
        running_max, weight_total, weighted_sum = loop_state
        block_start = block_index * ABLK
        block_latent = lax.dynamic_slice_in_dim(cache_latent, block_start, ABLK, 1)
        block_rope = lax.dynamic_slice_in_dim(cache_rope, block_start, ABLK, 1)
        scores = (
            jnp.einsum(
                "shc,skc->shk", query_latent, block_latent, preferred_element_type=jnp.float32
            )
            + jnp.einsum("shr,skr->shk", query_pe, block_rope, preferred_element_type=jnp.float32)
        ) * score_scale
        key_index = block_start + lax.iota(jnp.int32, ABLK)
        in_range = key_index[None, None, :] < lengths[:, None, None]
        scores = jnp.where(in_range, scores, masked_score)
        new_max = jnp.maximum(running_max, jnp.max(scores, axis=-1))
        rescale = jnp.exp(running_max - new_max)
        weights = jnp.exp(scores - new_max[..., None])
        weight_total = weight_total * rescale + jnp.sum(weights, axis=-1)
        weighted_sum = weighted_sum * rescale[..., None] + jnp.einsum(
            "shk,skc->shc",
            weights.astype(jnp.bfloat16),
            block_latent,
            preferred_element_type=jnp.float32,
        )
        return (new_max, weight_total, weighted_sum)

    longest = jnp.max(lengths)
    block_count = (longest + ABLK - 1) // ABLK
    ones_start = jnp.ones_like(new_score)
    sum_start = ones_start[..., None] * latent_new.astype(jnp.float32)[:, None, :]
    final_max, weight_total, weighted_sum = lax.fori_loop(
        0, block_count, attend_block, (new_score, ones_start, sum_start)
    )
    latent_out = (weighted_sum / weight_total[..., None]).astype(jnp.bfloat16)
    heads_out = (
        jnp.einsum("shc,chv->shv", latent_out, value_up, preferred_element_type=jnp.float32)
        .astype(jnp.bfloat16)
        .reshape(seq_count, -1)
    )
    column_rows = jnp.dot(
        lax.all_gather(heads_out, ("ep", "tp"), axis=0, tiled=True),
        out_proj,
        preferred_element_type=jnp.float32,
    ).astype(jnp.bfloat16)
    mixed_rows = lax.all_to_all(column_rows, ("ep", "tp"), split_axis=0, concat_axis=1, tiled=True)
    after_mix = (
        hidden_in.astype(jnp.float32)
        + gain_mix.astype(jnp.float32) * normalize(mixed_rows.astype(jnp.float32))
    ).astype(jnp.bfloat16)
    ffn_in = (normalize(after_mix.astype(jnp.float32)) * gain_ffn_in.astype(jnp.float32)).astype(
        jnp.bfloat16
    )
    affinity = jax.nn.sigmoid(jnp.dot(ffn_in, router, preferred_element_type=jnp.float32))
    experts_total = router.shape[1]
    own_start = lax.axis_index("tp") * seq_count
    own_routes = lax.dynamic_slice_in_dim(routes, own_start, seq_count, 0)
    choose = own_routes[..., None] == lax.iota(jnp.int32, experts_total)[None, None, :]
    chosen = jnp.sum(jnp.where(choose, affinity[:, None, :], 0.0), axis=-1)
    route_weights = chosen / jnp.sum(chosen, axis=-1, keepdims=True) * routed_scale
    group_rows, top_count = routes.shape
    capacity = 2 * ((group_rows * top_count + experts_total - 1) // experts_total)
    flat_routes = routes.reshape(-1)
    order_index = lax.iota(jnp.int32, group_rows * top_count)
    same_expert = flat_routes[:, None] == flat_routes[None, :]
    earlier = order_index[None, :] < order_index[:, None]
    slot_number = jnp.sum(jnp.logical_and(same_expert, earlier), axis=1)
    slot_number = slot_number.reshape(group_rows, top_count)
    own_slots = lax.dynamic_slice_in_dim(slot_number, own_start, seq_count, 0)
    slot_index = own_routes * capacity + own_slots
    slots_total = experts_total * capacity
    slot_table = jnp.any(
        slot_index[None, :, :] == lax.iota(jnp.int32, slots_total)[:, None, None], axis=-1
    ).astype(jnp.bfloat16)
    outgoing_terms = jnp.dot(slot_table, ffn_in, preferred_element_type=jnp.float32)
    outgoing = outgoing_terms.astype(jnp.bfloat16).reshape(experts_total, capacity, -1)
    received = lax.all_to_all(outgoing, ("ep", "tp"), split_axis=0, concat_axis=0, tiled=True)
    ep_count = lax.axis_size("ep")
    tp_count = lax.axis_size("tp")
    item_count = received.shape[1]
    width = received.shape[2]
    merged = jnp.sum(received.reshape(ep_count, tp_count, item_count, width), axis=1)
    outputs = swiglu(
        merged.reshape(ep_count * item_count, width), expert_gate[0], expert_up[0], expert_down[0]
    )
    copies = jnp.broadcast_to(
        outputs.reshape(ep_count, 1, item_count, width), (ep_count, tp_count, item_count, width)
    )
    copies = copies.reshape(ep_count * tp_count, item_count, width)
    returned = lax.all_to_all(copies, ("ep", "tp"), split_axis=0, concat_axis=0, tiled=True)
    picked = returned.reshape(slots_total, -1)[slot_index]
    routed = jnp.sum(picked.astype(jnp.float32) * route_weights[..., None], axis=1)
    shared = swiglu(ffn_in, shared_gate, shared_up, shared_down)
    combined = routed + shared.astype(jnp.float32)
    return (
        after_mix.astype(jnp.float32) + gain_ffn_out.astype(jnp.float32) * normalize(combined)
    ).astype(jnp.bfloat16)


def flip(index, mask, bits):
    result = 0
    for b in range(bits):
        bit = (index // 2**b) % 2
        result = result + (1 - bit if mask >> b & 1 else bit) * 2**b
    return result


def fused_kernel(
    ep_count,
    score_scale,
    hidden_hbm,
    qn_hbm,
    qr_hbm,
    nl_hbm,
    nr_hbm,
    len_hbm,
    routes_hbm,
    gm_hbm,
    gf_hbm,
    go_hbm,
    ab_hbm,
    cl_hbm,
    cr_hbm,
    vup_hbm,
    wo_hbm,
    router_hbm,
    eg_hbm,
    eu_hbm,
    ed_hbm,
    sg_hbm,
    su_hbm,
    sd_hbm,
    out_ref,
    hidden,
    qn,
    qr,
    nl,
    nr,
    length_of,
    route_of,
    gm,
    gf,
    go,
    ab,
    keys,
    rope_keys,
    vraw,
    wo,
    router,
    eg,
    eu,
    ed,
    sg,
    su,
    sd,
    vup,
    wq,
    new_keys,
    lat,
    xbuf,
    hbuf,
    cbuf,
    norm_rows,
    mix_rows,
    terms,
    back,
    local_sem,
    cache_sem,
    pair_send,
    pair_recv,
    ag_send,
    ag_recv,
):
    seq_count, heads, nope = qn.shape
    rope = qr.shape[2]
    width = out_ref.shape[1]
    latent = nl.shape[1]
    rows = seq_count * heads
    total_rows = ep_count * seq_count
    bits = (ep_count - 1).bit_length()
    me_e = lax.axis_index("ep")
    me_t = lax.axis_index("tp")

    def device(e, t):
        return {"ep": e, "tp": t}

    sibling = device(me_e, 1 - me_t)
    far_first = list(range(ep_count - 1, 0, -1))
    barrier = pltpu.get_barrier_semaphore()
    for target in [device(flip(me_e, mask, bits), me_t) for mask in far_first] + [sibling]:
        pl.semaphore_signal(
            barrier, inc=1, device_id=target, device_id_type=pl.DeviceIdType.MESH
        )

    started = []

    def fetch(source, target):
        copy = pltpu.make_async_copy(source, target, local_sem.at[len(started)])
        copy.start()
        started.append(copy)
        return copy

    len_copy = fetch(len_hbm, length_of)
    query_copies = [
        fetch(s, t) for s, t in ((qr_hbm, qr), (nl_hbm, nl), (nr_hbm, nr), (qn_hbm, qn))
    ]
    absorb_copy = fetch(ab_hbm, ab)
    value_copy = fetch(vup_hbm, vraw)
    rope_copy = fetch(cr_hbm, rope_keys)
    cache_copies = []
    for s in range(seq_count):
        copy = pltpu.make_async_copy(
            cl_hbm.at[s], keys.at[:, s * latent : (s + 1) * latent], cache_sem.at[s]
        )
        copy.start()
        cache_copies.append(copy)
    row_copies = [fetch(routes_hbm, route_of), fetch(hidden_hbm, hidden)]
    wo_copy = fetch(wo_hbm, wo.at[me_t])
    gain_copies = [fetch(s, t) for s, t in ((gm_hbm, gm), (gf_hbm, gf), (go_hbm, go))]
    router_copy = fetch(router_hbm, router)
    expert_copies = [
        fetch(s, t.at[me_t]) for s, t in ((eg_hbm, eg), (eu_hbm, eu), (ed_hbm, ed))
    ]
    shared_copies = [fetch(s, t) for s, t in ((sg_hbm, sg), (su_hbm, su), (sd_hbm, sd))]

    def to_sibling(index, source, target):
        return pltpu.make_async_remote_copy(
            src_ref=source,
            dst_ref=target.at[me_t],
            send_sem=pair_send.at[index],
            recv_sem=pair_recv.at[index],
            device_id=sibling,
            device_id_type=pl.DeviceIdType.MESH,
        )

    pair_copies = [
        to_sibling(index, source, target)
        for index, (source, target) in enumerate(
            ((wo_hbm, wo), (eg_hbm, eg), (eu_hbm, eu), (ed_hbm, ed))
        )
    ]

    value_dim = vraw.shape[2]
    step = 256 // heads
    order_row = lax.broadcasted_iota(jnp.int32, (256, 256), 0)
    order_lane = lax.broadcasted_iota(jnp.int32, (256, 256), 1)
    order = jnp.where(
        order_lane == order_row % step * heads + order_row // step, 1.0, 0.0
    ).astype(jnp.bfloat16)

    half = rope // 2
    turn_row = lax.broadcasted_iota(jnp.int32, (seq_count, rope), 0)
    turn_lane = lax.broadcasted_iota(jnp.int32, (seq_count, rope), 1)
    inverse = jnp.zeros((seq_count, rope), jnp.float32)
    for i in range(half):
        inverse = jnp.where(turn_lane % half == i, rope_theta ** (-2.0 * i / rope), inverse)
    len_copy.wait()
    position = jnp.zeros((seq_count, rope), jnp.float32)
    for s in range(seq_count):
        position = jnp.where(turn_row == s, length_of[s].astype(jnp.float32), position)
    angles = position * inverse
    cosine = jnp.cos(angles)
    sine = jnp.sin(angles) * jnp.where(turn_lane < half, -1.0, 1.0)

    def turned(values, cos_rows, sin_rows):
        swapped = jnp.concatenate([values[:, half:], values[:, :half]], axis=1)
        return values * cos_rows + swapped * sin_rows

    def per_head(table):
        return jnp.broadcast_to(table[:, None, :], (seq_count, heads, rope)).reshape(rows, rope)

    for copy in query_copies:
        copy.wait()
    query_rows = qr[...].astype(jnp.float32).reshape(rows, rope)
    q_pe = turned(query_rows, per_head(cosine), per_head(sine))
    key_rows = turned(nr[...].astype(jnp.float32), cosine, sine)
    new_rows = normalize(nl[...].astype(jnp.float32)).astype(jnp.bfloat16).astype(jnp.float32)
    rope_at = seq_count * latent
    new_keys[...] = jnp.zeros_like(new_keys)
    for s in range(seq_count):
        new_keys[0:1, s * latent : (s + 1) * latent] = new_rows[s : s + 1, :]
    new_keys[0:1, rope_at:] = jnp.concatenate(
        [key_rows[s : s + 1, :] for s in range(seq_count)], axis=1
    )

    nope_rows = qn[...].astype(jnp.float32).reshape(rows, nope)
    row_head = lax.broadcasted_iota(jnp.int32, (rows, 2 * nope), 0) % heads
    pair_lane = lax.broadcasted_iota(jnp.int32, (rows, 2 * nope), 1) // nope
    doubled = jnp.concatenate([nope_rows, nope_rows], axis=1)
    spread_query = jnp.concatenate(
        [
            jnp.where(row_head == pair_lane + 2 * j, doubled, 0.0).astype(jnp.bfloat16)
            for j in range(heads // 2)
        ],
        axis=1,
    )
    absorb_copy.wait()
    q_lat = jnp.dot(spread_query, ab[...], preferred_element_type=jnp.float32)
    q_turned = q_lat.T
    lane_seq = lax.broadcasted_iota(jnp.int32, (latent, rows), 1) // heads
    for s in range(seq_count):
        wq[s * latent : (s + 1) * latent, :] = jnp.where(lane_seq == s, q_turned, 0.0).astype(
            jnp.bfloat16
        )
    rope_turned = jnp.concatenate([q_pe] * (128 // rope), axis=1).T[:rope]
    rope_seq = lax.broadcasted_iota(jnp.int32, (rope, rows), 1) // heads
    for s in range(seq_count):
        wq[rope_at + s * rope : rope_at + (s + 1) * rope, :] = jnp.where(
            rope_seq == s, rope_turned, 0.0
        ).astype(jnp.bfloat16)

    value_copy.wait()
    for b in range(0, latent // step, 2):
        blocks = [
            vraw[i * step : (i + 1) * step].reshape(step * heads, value_dim) for i in (b, b + 1)
        ]
        ordered = jnp.dot(
            order, jnp.concatenate(blocks, axis=1), preferred_element_type=jnp.float32
        ).astype(jnp.bfloat16)
        for i in range(2):
            for h in range(heads):
                vup[(b + i) * step : (b + i + 1) * step, h * value_dim : (h + 1) * value_dim] = (
                    ordered[h * step : (h + 1) * step, i * value_dim : (i + 1) * value_dim]
                )

    context = keys.shape[0]
    rope_copy.wait()
    keys[:, rope_at:] = rope_keys[...].T
    for copy in cache_copies:
        copy.wait()
    lengths_row = jnp.zeros((1, rows), jnp.int32)
    lane_of = lax.broadcasted_iota(jnp.int32, (1, rows), 1) // heads
    for s in range(seq_count):
        lengths_row = jnp.where(lane_of == s, length_of[s], lengths_row)
    new_score = (
        jnp.dot(new_keys[...].astype(jnp.bfloat16), wq[...], preferred_element_type=jnp.float32)[
            0:1
        ]
        * score_scale
    )
    scores = jnp.dot(keys[...], wq[...], preferred_element_type=jnp.float32) * score_scale
    key_index = lax.broadcasted_iota(jnp.int32, (context, rows), 0)
    scores = jnp.where(key_index < lengths_row, scores, masked_score)
    row_max = jnp.maximum(jnp.max(scores, axis=0, keepdims=True), new_score)
    weights = jnp.exp(scores - row_max)
    new_weight = jnp.exp(new_score - row_max)
    weight_total = jnp.sum(weights, axis=0, keepdims=True) + new_weight
    new_weight = new_weight.astype(jnp.bfloat16).astype(jnp.float32)
    turned_weights = weights.astype(jnp.bfloat16).T
    side = jnp.concatenate(
        [weight_total, new_weight, jnp.zeros((6, rows), jnp.float32)], axis=0
    ).T
    for s in range(seq_count):
        part = slice(s * heads, (s + 1) * heads)
        weighted = jnp.dot(
            turned_weights[part],
            keys[:, s * latent : (s + 1) * latent],
            preferred_element_type=jnp.float32,
        )
        weighted = weighted + side[part, 1:2] * new_rows[s : s + 1, :]
        lat[part, :] = (weighted / side[part, 0:1]).astype(jnp.bfloat16)

    spread = jnp.dot(lat[...], vup[...], preferred_element_type=jnp.float32)
    own_heads = []
    head_row = lax.broadcasted_iota(jnp.int32, (seq_count, heads, value_dim), 1)
    for h in range(heads):
        block = spread[:, h * value_dim : (h + 1) * value_dim].reshape(seq_count, heads, value_dim)
        own_heads.append(jnp.sum(jnp.where(head_row == h, block, 0.0), axis=1))
    hbuf[me_e] = jnp.concatenate(own_heads, axis=1).astype(jnp.bfloat16)

    for copy in row_copies:
        copy.wait()
    xbuf[me_e, :, 0:width] = hidden[...]
    mark_shape = (seq_count, xbuf.shape[2] - width)
    mark_row = lax.broadcasted_iota(jnp.int32, mark_shape, 0)
    mark_lane = lax.broadcasted_iota(jnp.int32, mark_shape, 1)
    marks = jnp.zeros(mark_shape, jnp.float32)
    for s in range(seq_count):
        for j in range(route_of.shape[0]):
            expert = route_of[j, me_t * seq_count + s]
            marks = jnp.where((mark_row == s) & (mark_lane == expert), 1.0, marks)
    xbuf[me_e, :, width:] = marks.astype(jnp.bfloat16)

    pending = []

    def remote(which, mask, source, target, to):
        return pltpu.make_async_remote_copy(
            src_ref=source,
            dst_ref=target,
            send_sem=ag_send.at[which, mask],
            recv_sem=ag_recv.at[which, to],
            device_id=device(flip(me_e, mask, bits), me_t),
            device_id_type=pl.DeviceIdType.MESH,
        )

    def share(which, buf):
        for mask in far_first:
            copy = remote(which, mask, buf.at[me_e], buf.at[me_e], me_e)
            copy.start()
            pending.append(copy)

    def arrive(which, buf, mask):
        e = flip(me_e, mask, bits)
        remote(which, mask, buf.at[e], buf.at[e], e).wait_recv()

    pl.semaphore_wait(barrier, ep_count)
    share(1, hbuf)
    share(0, xbuf)
    for copy in pair_copies:
        copy.start()
    wo_copy.wait()
    pair_copies[0].wait_recv()
    for mask in reversed(far_first):
        arrive(1, hbuf, mask)

    flat_heads = hbuf[...].reshape(total_rows, hbuf.shape[2])
    cbuf[me_e] = jnp.concatenate(
        [jnp.dot(flat_heads, wo[t], preferred_element_type=jnp.float32) for t in range(2)], axis=1
    ).astype(jnp.bfloat16)
    share(2, cbuf)
    for mask in reversed(far_first):
        arrive(0, xbuf, mask)
    for copy in gain_copies + [router_copy] + expert_copies:
        copy.wait()
    for copy in pair_copies[1:]:
        copy.wait_recv()
    for mask in reversed(far_first):
        arrive(2, cbuf, mask)

    gains = [ref[...].astype(jnp.float32).reshape(1, width) for ref in (gm, gf, go)]
    mixed = jnp.concatenate([cbuf[o] for o in range(ep_count)], axis=1).astype(jnp.float32)
    stage = xbuf[...].reshape(total_rows, xbuf.shape[2])
    after_mix = (stage[:, :width].astype(jnp.float32) + gains[0] * normalize(mixed)).astype(
        jnp.bfloat16
    )
    mix_rows[...] = after_mix.reshape(mix_rows.shape)
    ffn_in = (normalize(after_mix.astype(jnp.float32)) * gains[1]).astype(jnp.bfloat16)
    norm_rows[...] = ffn_in.reshape(norm_rows.shape)
    affinity = jax.nn.sigmoid(
        lax.dot_general(
            ffn_in, router[...], (((1,), (1,)), ((), ())), preferred_element_type=jnp.float32
        )
    )
    hot = stage[:, width : width + affinity.shape[1]].astype(jnp.float32)
    chosen = affinity * hot
    lane = lax.broadcasted_iota(jnp.int32, chosen.shape, 1)
    whole = jnp.sum(chosen, axis=1, keepdims=True)
    outcome = jnp.zeros((total_rows, width), jnp.float32)
    for t in range(2):
        mine = jnp.sum(jnp.where(lane == me_e * 2 + t, chosen, 0.0), axis=1, keepdims=True)
        mine = mine / whole * routed_scale
        expert_out = swiglu(ffn_in, eg[t], eu[t], ed[t])
        outcome = outcome + expert_out.astype(jnp.float32) * mine
    terms[...] = outcome.astype(jnp.bfloat16).reshape(terms.shape)
    for mask in far_first:
        copy = remote(3, mask, terms.at[flip(me_e, mask, bits)], back.at[me_e], me_e)
        copy.start()
        pending.append(copy)
    for copy in shared_copies:
        copy.wait()
    combined = terms[me_e].astype(jnp.float32) + swiglu(
        norm_rows[me_e], sg[...], su[...], sd[...]
    ).astype(jnp.float32)
    for mask in reversed(far_first):
        arrive(3, back, mask)
        combined = combined + back[flip(me_e, mask, bits)].astype(jnp.float32)
    out_ref[...] = (
        mix_rows[me_e].astype(jnp.float32) + gains[2] * normalize(combined)
    ).astype(jnp.bfloat16)
    for copy in pending + pair_copies:
        copy.wait_send()


def local_fused(
    hidden_in,
    query_nope,
    query_rope,
    new_latent,
    new_rope,
    cache_latent,
    cache_rope,
    lengths,
    absorb_key,
    value_up,
    out_proj,
    gain_mix,
    gain_ffn_in,
    router,
    routes,
    expert_gate,
    expert_up,
    expert_down,
    shared_gate,
    shared_up,
    shared_down,
    gain_ffn_out,
):
    seq_count, width = hidden_in.shape
    heads, latent = query_nope.shape[1], cache_latent.shape[2]
    context, rope = cache_rope.shape[1:]
    ep_count = lax.axis_size("ep")
    bf = jnp.bfloat16
    score_scale = (query_nope.shape[-1] + query_rope.shape[-1]) ** (-0.5)
    dma = pltpu.SemaphoreType.DMA
    total_rows = ep_count * seq_count
    rows = seq_count * heads
    depth = seq_count * (latent + rope)
    rope_rows = jnp.swapaxes(cache_rope, 1, 2).reshape(seq_count * rope, context)
    router_rows = jnp.swapaxes(router, 0, 1)
    absorb_rows = jnp.transpose(absorb_key, (1, 2, 0)).reshape(-1, latent)
    route_rows = jnp.swapaxes(routes, 0, 1)
    gate, up, down = expert_gate[0], expert_up[0], expert_down[0]
    operands = (
        hidden_in,
        query_nope,
        query_rope,
        new_latent,
        new_rope,
        lengths,
        route_rows,
        gain_mix,
        gain_ffn_in,
        gain_ffn_out,
        absorb_rows,
        cache_latent,
        rope_rows,
        value_up,
        out_proj,
        router_rows,
        gate,
        up,
        down,
        shared_gate,
        shared_up,
        shared_down,
    )

    def near(array, lead=()):
        return pltpu.VMEM(lead + array.shape, array.dtype)

    flops = 2 * total_rows * width * out_proj.shape[1]
    return pl.pallas_call(
        functools.partial(fused_kernel, ep_count, score_scale),
        out_shape=jax.ShapeDtypeStruct((seq_count, width), bf),
        in_specs=[pl.BlockSpec(memory_space=pl.ANY)] * len(operands),
        out_specs=pl.BlockSpec(memory_space=pltpu.VMEM),
        scratch_shapes=[near(a) for a in operands[:5]]
        + [pltpu.SMEM(lengths.shape, jnp.int32), pltpu.SMEM(route_rows.shape, jnp.int32)]
        + [near(a) for a in operands[7:11]]
        + [
            pltpu.VMEM((context, depth), bf),
            near(rope_rows),
            near(value_up),
            near(out_proj, (2,)),
            near(router_rows),
            near(gate, (2,)),
            near(up, (2,)),
            near(down, (2,)),
            near(shared_gate),
            near(shared_up),
            near(shared_down),
            pltpu.VMEM((latent, heads * value_up.shape[2]), bf),
            pltpu.VMEM((depth, rows), bf),
            pltpu.VMEM((8, depth), jnp.float32),
            pltpu.VMEM((rows, latent), bf),
            pltpu.VMEM((ep_count, seq_count, width + 128), bf),
            pltpu.VMEM((ep_count, seq_count, out_proj.shape[0]), bf),
            pltpu.VMEM((ep_count, total_rows, 2 * out_proj.shape[1]), bf),
            pltpu.VMEM((ep_count, seq_count, width), bf),
            pltpu.VMEM((ep_count, seq_count, width), bf),
            pltpu.VMEM((ep_count, seq_count, width), bf),
            pltpu.VMEM((ep_count, seq_count, width), bf),
            dma((len(operands),)),
            dma((seq_count,)),
            dma((4,)),
            dma((4,)),
            dma((4, ep_count)),
            dma((4, ep_count)),
        ],
        compiler_params=pltpu.CompilerParams(
            collective_id=0, has_side_effects=True, vmem_limit_bytes=56 * 2**20
        ),
        cost_estimate=pl.CostEstimate(flops=flops, bytes_accessed=2**24, transcendentals=0),
        name="layer_step",
    )(*operands)


def local(*args):
    hidden_in, out_proj, router = args[0], args[10], args[13]
    device_count = lax.axis_size("ep") * lax.axis_size("tp")
    ep_count = lax.axis_size("ep")
    fits = (
        lax.axis_size("tp") == 2
        and ep_count & (ep_count - 1) == 0
        and hidden_in.shape[0] == 8
        and args[1].shape[1] == 16
        and device_count * hidden_in.shape[0] <= 256
        and out_proj.shape[1] % 128 == 0
        and router.shape[1] == device_count
    )
    return local_fused(*args) if fits else local_wide(*args)


def solution(mesh):
    placed = (
        P(("grp", "ep", "tp"), None),
        P(("grp", "ep", "tp"), None, None),
        P(("grp", "ep", "tp"), None, None),
        P(("grp", "ep", "tp"), None),
        P(("grp", "ep", "tp"), None),
        P(("grp", "ep", "tp"), None, None),
        P(("grp", "ep", "tp"), None, None),
        P(("grp", "ep", "tp")),
        P(),
        P(),
        P(None, ("ep", "tp")),
        P(),
        P(),
        P(),
        P(("grp", "ep"), None),
        P(("ep", "tp"), None, None),
        P(("ep", "tp"), None, None),
        P(("ep", "tp"), None, None),
        P(),
        P(),
        P(),
        P(),
    )
    return jax.shard_map(
        local, mesh=mesh, in_specs=placed, out_specs=P(("grp", "ep", "tp"), None), check_vma=False
    )
```

```python
import functools
import math

import jax
import jax.numpy as jnp
from jax import lax
from jax.experimental import pallas as pl
from jax.experimental.pallas import tpu as pltpu
from jax.sharding import PartitionSpec as P

ABLK = 512


rope_theta = 10000.0
norm_eps = 1e-06
routed_scale = 2.5
masked_score = -1e30


def normalize(values):
    return values * lax.rsqrt(jnp.mean(values * values, axis=-1, keepdims=True) + norm_eps)


def rotate(values, positions):
    half_dim = values.shape[-1] // 2
    inverse = rope_theta ** (-jnp.arange(half_dim, dtype=jnp.float32) * 2.0 / values.shape[-1])
    angles = positions * inverse
    cosine = jnp.cos(angles)
    sine_table = jnp.sin(angles)
    first_half = values[..., :half_dim]
    second_half = values[..., half_dim:]
    return jnp.concatenate(
        [
            first_half * cosine - second_half * sine_table,
            first_half * sine_table + second_half * cosine,
        ],
        axis=-1,
    )


def swiglu(flat_rows, gate_w, up_w, down_w):
    gate_part = jnp.dot(flat_rows, gate_w, preferred_element_type=jnp.float32)
    up_part = jnp.dot(flat_rows, up_w, preferred_element_type=jnp.float32)
    inner_rows = (jax.nn.silu(gate_part) * up_part).astype(jnp.bfloat16)
    return jnp.dot(inner_rows, down_w, preferred_element_type=jnp.float32).astype(jnp.bfloat16)


def local_wide(
    hidden_in,
    query_nope,
    query_rope,
    new_latent,
    new_rope,
    cache_latent,
    cache_rope,
    lengths,
    absorb_key,
    value_up,
    out_proj,
    gain_mix,
    gain_ffn_in,
    router,
    routes,
    expert_gate,
    expert_up,
    expert_down,
    shared_gate,
    shared_up,
    shared_down,
    gain_ffn_out,
):
    seq_count = hidden_in.shape[0]
    positions = lengths.astype(jnp.float32)
    query_latent = jnp.einsum(
        "shn,chn->shc", query_nope, absorb_key, preferred_element_type=jnp.float32
    ).astype(jnp.bfloat16)
    query_pe = rotate(query_rope.astype(jnp.float32), positions[:, None, None]).astype(jnp.bfloat16)
    latent_new = normalize(new_latent.astype(jnp.float32)).astype(jnp.bfloat16)
    key_new = rotate(new_rope.astype(jnp.float32), positions[:, None]).astype(jnp.bfloat16)
    score_scale = (query_nope.shape[-1] + query_rope.shape[-1]) ** (-0.5)
    new_score = (
        jnp.einsum("shc,sc->sh", query_latent, latent_new, preferred_element_type=jnp.float32)
        + jnp.einsum("shr,sr->sh", query_pe, key_new, preferred_element_type=jnp.float32)
    ) * score_scale

    def attend_block(block_index, loop_state):
        running_max, weight_total, weighted_sum = loop_state
        block_start = block_index * ABLK
        block_latent = lax.dynamic_slice_in_dim(cache_latent, block_start, ABLK, 1)
        block_rope = lax.dynamic_slice_in_dim(cache_rope, block_start, ABLK, 1)
        scores = (
            jnp.einsum(
                "shc,skc->shk", query_latent, block_latent, preferred_element_type=jnp.float32
            )
            + jnp.einsum("shr,skr->shk", query_pe, block_rope, preferred_element_type=jnp.float32)
        ) * score_scale
        key_index = block_start + lax.iota(jnp.int32, ABLK)
        in_range = key_index[None, None, :] < lengths[:, None, None]
        scores = jnp.where(in_range, scores, masked_score)
        new_max = jnp.maximum(running_max, jnp.max(scores, axis=-1))
        rescale = jnp.exp(running_max - new_max)
        weights = jnp.exp(scores - new_max[..., None])
        weight_total = weight_total * rescale + jnp.sum(weights, axis=-1)
        weighted_sum = weighted_sum * rescale[..., None] + jnp.einsum(
            "shk,skc->shc",
            weights.astype(jnp.bfloat16),
            block_latent,
            preferred_element_type=jnp.float32,
        )
        return (new_max, weight_total, weighted_sum)

    longest = jnp.max(lengths)
    block_count = (longest + ABLK - 1) // ABLK
    ones_start = jnp.ones_like(new_score)
    sum_start = ones_start[..., None] * latent_new.astype(jnp.float32)[:, None, :]
    final_max, weight_total, weighted_sum = lax.fori_loop(
        0, block_count, attend_block, (new_score, ones_start, sum_start)
    )
    latent_out = (weighted_sum / weight_total[..., None]).astype(jnp.bfloat16)
    heads_out = (
        jnp.einsum("shc,chv->shv", latent_out, value_up, preferred_element_type=jnp.float32)
        .astype(jnp.bfloat16)
        .reshape(seq_count, -1)
    )
    column_rows = jnp.dot(
        lax.all_gather(heads_out, ("ep", "tp"), axis=0, tiled=True),
        out_proj,
        preferred_element_type=jnp.float32,
    ).astype(jnp.bfloat16)
    mixed_rows = lax.all_to_all(column_rows, ("ep", "tp"), split_axis=0, concat_axis=1, tiled=True)
    after_mix = (
        hidden_in.astype(jnp.float32)
        + gain_mix.astype(jnp.float32) * normalize(mixed_rows.astype(jnp.float32))
    ).astype(jnp.bfloat16)
    ffn_in = (normalize(after_mix.astype(jnp.float32)) * gain_ffn_in.astype(jnp.float32)).astype(
        jnp.bfloat16
    )
    affinity = jax.nn.sigmoid(jnp.dot(ffn_in, router, preferred_element_type=jnp.float32))
    experts_total = router.shape[1]
    own_start = lax.axis_index("tp") * seq_count
    own_routes = lax.dynamic_slice_in_dim(routes, own_start, seq_count, 0)
    choose = own_routes[..., None] == lax.iota(jnp.int32, experts_total)[None, None, :]
    chosen = jnp.sum(jnp.where(choose, affinity[:, None, :], 0.0), axis=-1)
    route_weights = chosen / jnp.sum(chosen, axis=-1, keepdims=True) * routed_scale
    group_rows, top_count = routes.shape
    capacity = 2 * ((group_rows * top_count + experts_total - 1) // experts_total)
    flat_routes = routes.reshape(-1)
    order_index = lax.iota(jnp.int32, group_rows * top_count)
    same_expert = flat_routes[:, None] == flat_routes[None, :]
    earlier = order_index[None, :] < order_index[:, None]
    slot_number = jnp.sum(jnp.logical_and(same_expert, earlier), axis=1)
    slot_number = slot_number.reshape(group_rows, top_count)
    own_slots = lax.dynamic_slice_in_dim(slot_number, own_start, seq_count, 0)
    slot_index = own_routes * capacity + own_slots
    slots_total = experts_total * capacity
    slot_table = jnp.any(
        slot_index[None, :, :] == lax.iota(jnp.int32, slots_total)[:, None, None], axis=-1
    ).astype(jnp.bfloat16)
    outgoing_terms = jnp.dot(slot_table, ffn_in, preferred_element_type=jnp.float32)
    outgoing = outgoing_terms.astype(jnp.bfloat16).reshape(experts_total, capacity, -1)
    received = lax.all_to_all(outgoing, ("ep", "tp"), split_axis=0, concat_axis=0, tiled=True)
    ep_count = lax.axis_size("ep")
    tp_count = lax.axis_size("tp")
    item_count = received.shape[1]
    width = received.shape[2]
    merged = jnp.sum(received.reshape(ep_count, tp_count, item_count, width), axis=1)
    outputs = swiglu(
        merged.reshape(ep_count * item_count, width), expert_gate[0], expert_up[0], expert_down[0]
    )
    copies = jnp.broadcast_to(
        outputs.reshape(ep_count, 1, item_count, width), (ep_count, tp_count, item_count, width)
    )
    copies = copies.reshape(ep_count * tp_count, item_count, width)
    returned = lax.all_to_all(copies, ("ep", "tp"), split_axis=0, concat_axis=0, tiled=True)
    picked = returned.reshape(slots_total, -1)[slot_index]
    routed = jnp.sum(picked.astype(jnp.float32) * route_weights[..., None], axis=1)
    shared = swiglu(ffn_in, shared_gate, shared_up, shared_down)
    combined = routed + shared.astype(jnp.float32)
    return (
        after_mix.astype(jnp.float32) + gain_ffn_out.astype(jnp.float32) * normalize(combined)
    ).astype(jnp.bfloat16)


def flip(index, mask, bits):
    result = 0
    for b in range(bits):
        bit = (index // 2**b) % 2
        result = result + (1 - bit if mask >> b & 1 else bit) * 2**b
    return result


def fused_kernel(
    ep_count,
    score_scale,
    hidden_hbm,
    qn_hbm,
    qr_hbm,
    nl_hbm,
    nr_hbm,
    len_hbm,
    routes_hbm,
    gm_hbm,
    gf_hbm,
    go_hbm,
    ab_hbm,
    cl_hbm,
    cr_hbm,
    vup_hbm,
    wo_hbm,
    router_hbm,
    eg_hbm,
    eu_hbm,
    ed_hbm,
    sg_hbm,
    su_hbm,
    sd_hbm,
    out_ref,
    hidden,
    qn,
    qr,
    nl,
    nr,
    length_of,
    route_of,
    gm,
    gf,
    go,
    ab,
    keys,
    rope_keys,
    vraw,
    wo,
    router,
    eg,
    eu,
    ed,
    sg,
    su,
    sd,
    vup,
    wq,
    new_keys,
    lat,
    xbuf,
    hbuf,
    cbuf,
    norm_rows,
    mix_rows,
    terms,
    back,
    local_sem,
    cache_sem,
    pair_send,
    pair_recv,
    ag_send,
    ag_recv,
    ready,
    scores,
    turned_weights,
):
    seq_count, heads, nope = qn.shape
    rope = qr.shape[2]
    width = out_ref.shape[1]
    latent = nl.shape[1]
    rows = seq_count * heads
    total_rows = ep_count * seq_count
    bits = (ep_count - 1).bit_length()
    me_e = lax.axis_index("ep")
    me_t = lax.axis_index("tp")

    def device(e, t):
        return {"ep": e, "tp": t}

    sibling = device(me_e, 1 - me_t)
    far_first = list(range(ep_count - 1, 0, -1))
    barrier = pltpu.get_barrier_semaphore()

    def tell(semaphore, target):
        pl.semaphore_signal(
            semaphore, inc=1, device_id=target, device_id_type=pl.DeviceIdType.MESH
        )

    @pl.when(me_t == 1)
    def _():
        tell(barrier, sibling)

    started = []

    def fetch(source, target):
        copy = pltpu.make_async_copy(source, target, local_sem.at[len(started)])
        copy.start()
        started.append(copy)
        return copy

    len_copy = fetch(len_hbm, length_of)
    query_copies = [
        fetch(s, t) for s, t in ((qr_hbm, qr), (nl_hbm, nl), (nr_hbm, nr), (qn_hbm, qn))
    ]
    absorb_copy = fetch(ab_hbm, ab)
    value_copy = fetch(vup_hbm, vraw)
    rope_copy = fetch(cr_hbm, rope_keys)
    cache_copies = []
    for s in range(seq_count):
        copy = pltpu.make_async_copy(
            cl_hbm.at[s], keys.at[:, s * latent : (s + 1) * latent], cache_sem.at[s]
        )
        copy.start()
        cache_copies.append(copy)
    def to_sibling(index, source, target):
        return pltpu.make_async_remote_copy(
            src_ref=source,
            dst_ref=target.at[me_t],
            send_sem=pair_send.at[index],
            recv_sem=pair_recv.at[index],
            device_id=sibling,
            device_id_type=pl.DeviceIdType.MESH,
        )

    pair_copies = [
        to_sibling(index, source, target)
        for index, (source, target) in enumerate(
            ((wo_hbm, wo), (eg_hbm, eg), (eu_hbm, eu), (ed_hbm, ed))
        )
    ]

    @pl.when(me_t == 0)
    def _():
        pl.semaphore_wait(barrier, 1)
        tell(ready.at[0], sibling)

    @pl.when(me_t == 1)
    def _():
        pl.semaphore_wait(ready.at[0], 1)
        for mask in far_first:
            tell(barrier, device(flip(me_e, mask, bits), me_t))

    for copy in pair_copies:
        copy.start()

    value_dim = vraw.shape[2]
    step = 256 // heads
    order_row = lax.broadcasted_iota(jnp.int32, (256, 256), 0)
    order_lane = lax.broadcasted_iota(jnp.int32, (256, 256), 1)
    order = jnp.where(
        order_lane == order_row % step * heads + order_row // step, 1.0, 0.0
    ).astype(jnp.bfloat16)

    half = rope // 2
    turn_row = lax.broadcasted_iota(jnp.int32, (seq_count, rope), 0)
    turn_lane = lax.broadcasted_iota(jnp.int32, (seq_count, rope), 1)
    inverse = jnp.zeros((seq_count, rope), jnp.float32)
    for i in range(half):
        inverse = jnp.where(turn_lane % half == i, rope_theta ** (-2.0 * i / rope), inverse)
    len_copy.wait()
    position = jnp.zeros((seq_count, rope), jnp.float32)
    for s in range(seq_count):
        position = jnp.where(turn_row == s, length_of[s].astype(jnp.float32), position)
    angles = position * inverse
    cosine = jnp.cos(angles)
    sine = jnp.sin(angles) * jnp.where(turn_lane < half, -1.0, 1.0)

    def turned(values, cos_rows, sin_rows):
        swapped = jnp.concatenate([values[:, half:], values[:, :half]], axis=1)
        return values * cos_rows + swapped * sin_rows

    def per_head(table):
        return jnp.broadcast_to(table[:, None, :], (seq_count, heads, rope)).reshape(rows, rope)

    for copy in query_copies:
        copy.wait()
    query_rows = qr[...].astype(jnp.float32).reshape(rows, rope)
    q_pe = turned(query_rows, per_head(cosine), per_head(sine))
    key_rows = turned(nr[...].astype(jnp.float32), cosine, sine)
    new_rows = normalize(nl[...].astype(jnp.float32)).astype(jnp.bfloat16).astype(jnp.float32)
    rope_at = seq_count * latent
    new_keys[...] = jnp.zeros_like(new_keys)
    for s in range(seq_count):
        new_keys[0:1, s * latent : (s + 1) * latent] = new_rows[s : s + 1, :]
    new_keys[0:1, rope_at:] = jnp.concatenate(
        [key_rows[s : s + 1, :] for s in range(seq_count)], axis=1
    )

    nope_rows = qn[...].astype(jnp.float32).reshape(rows, nope)
    row_head = lax.broadcasted_iota(jnp.int32, (rows, 2 * nope), 0) % heads
    pair_lane = lax.broadcasted_iota(jnp.int32, (rows, 2 * nope), 1) // nope
    doubled = jnp.concatenate([nope_rows, nope_rows], axis=1)
    spread_query = jnp.concatenate(
        [
            jnp.where(row_head == pair_lane + 2 * j, doubled, 0.0).astype(jnp.bfloat16)
            for j in range(heads // 2)
        ],
        axis=1,
    )
    absorb_copy.wait()
    q_lat = jnp.dot(spread_query, ab[...], preferred_element_type=jnp.float32)
    q_turned = q_lat.T
    lane_seq = lax.broadcasted_iota(jnp.int32, (latent, rows), 1) // heads
    for s in range(seq_count):
        wq[s * latent : (s + 1) * latent, :] = jnp.where(lane_seq == s, q_turned, 0.0).astype(
            jnp.bfloat16
        )
    rope_turned = jnp.concatenate([q_pe] * (128 // rope), axis=1).T[:rope]
    rope_seq = lax.broadcasted_iota(jnp.int32, (rope, rows), 1) // heads
    for s in range(seq_count):
        wq[rope_at + s * rope : rope_at + (s + 1) * rope, :] = jnp.where(
            rope_seq == s, rope_turned, 0.0
        ).astype(jnp.bfloat16)

    value_copy.wait()
    for b in range(0, latent // step, 2):
        blocks = [
            vraw[i * step : (i + 1) * step].reshape(step * heads, value_dim) for i in (b, b + 1)
        ]
        ordered = jnp.dot(
            order, jnp.concatenate(blocks, axis=1), preferred_element_type=jnp.float32
        ).astype(jnp.bfloat16)
        for i in range(2):
            for h in range(heads):
                vup[(b + i) * step : (b + i + 1) * step, h * value_dim : (h + 1) * value_dim] = (
                    ordered[h * step : (h + 1) * step, i * value_dim : (i + 1) * value_dim]
                )

    context = keys.shape[0]
    rope_copy.wait()
    keys[:, rope_at:] = rope_keys[...].T
    lengths_row = jnp.zeros((1, rows), jnp.int32)
    lane_of = lax.broadcasted_iota(jnp.int32, (1, rows), 1) // heads
    for s in range(seq_count):
        lengths_row = jnp.where(lane_of == s, length_of[s], lengths_row)
    new_score = jnp.dot(
        new_keys[...].astype(jnp.bfloat16), wq[...], preferred_element_type=jnp.float32
    )[0:1]
    for copy in cache_copies:
        copy.wait()
    row_copies = [fetch(routes_hbm, route_of), fetch(hidden_hbm, hidden)]
    wo_copy = fetch(wo_hbm, wo.at[me_t])
    gain_copies = [fetch(s, t) for s, t in ((gm_hbm, gm), (gf_hbm, gf), (go_hbm, go))]
    router_copy = fetch(router_hbm, router)
    expert_copies = [
        fetch(s, t.at[me_t]) for s, t in ((eg_hbm, eg), (eu_hbm, eu), (ed_hbm, ed))
    ]
    shared_copies = [fetch(s, t) for s, t in ((sg_hbm, sg), (su_hbm, su), (sd_hbm, sd))]

    block = 256
    key_index = lax.broadcasted_iota(jnp.int32, (block, rows), 0)
    tops = jnp.full((8, rows), masked_score, jnp.float32)
    for k in range(0, context, block):
        found = jnp.dot(keys[k : k + block, :], wq[...], preferred_element_type=jnp.float32)
        found = jnp.where(key_index < lengths_row - k, found, masked_score)
        scores[k : k + block, :] = found
        tops = jnp.maximum(tops, jnp.max(found.reshape(block // 8, 8, rows), axis=0))
    row_max = jnp.maximum(jnp.max(tops, axis=0, keepdims=True), new_score)
    power = score_scale * math.log2(math.e)
    sums = jnp.zeros((8, rows), jnp.float32)
    for k in range(0, context, block):
        weights = jnp.exp2((scores[k : k + block, :] - row_max) * power)
        sums = sums + jnp.sum(weights.reshape(block // 8, 8, rows), axis=0)
        turned_weights[:, k : k + block] = weights.astype(jnp.bfloat16).T
    new_weight = jnp.exp2((new_score - row_max) * power)
    weight_total = jnp.sum(sums, axis=0, keepdims=True) + new_weight
    new_weight = new_weight.astype(jnp.bfloat16).astype(jnp.float32)
    side = jnp.concatenate(
        [weight_total, new_weight, jnp.zeros((6, rows), jnp.float32)], axis=0
    ).T
    for s in range(seq_count):
        part = slice(s * heads, (s + 1) * heads)
        weighted = jnp.dot(
            turned_weights[part, :],
            keys[:, s * latent : (s + 1) * latent],
            preferred_element_type=jnp.float32,
        )
        weighted = weighted + side[part, 1:2] * new_rows[s : s + 1, :]
        lat[part, :] = (weighted / side[part, 0:1]).astype(jnp.bfloat16)

    spread = jnp.dot(lat[...], vup[...], preferred_element_type=jnp.float32)
    own_heads = []
    head_row = lax.broadcasted_iota(jnp.int32, (seq_count, heads, value_dim), 1)
    for h in range(heads):
        block = spread[:, h * value_dim : (h + 1) * value_dim].reshape(seq_count, heads, value_dim)
        own_heads.append(jnp.sum(jnp.where(head_row == h, block, 0.0), axis=1))
    hbuf[me_e] = jnp.concatenate(own_heads, axis=1).astype(jnp.bfloat16)

    for copy in row_copies:
        copy.wait()
    xbuf[me_e, :, 0:width] = hidden[...]
    mark_shape = (seq_count, xbuf.shape[2] - width)
    mark_row = lax.broadcasted_iota(jnp.int32, mark_shape, 0)
    mark_lane = lax.broadcasted_iota(jnp.int32, mark_shape, 1)
    marks = jnp.zeros(mark_shape, jnp.float32)
    for s in range(seq_count):
        for j in range(route_of.shape[0]):
            expert = route_of[j, me_t * seq_count + s]
            marks = jnp.where((mark_row == s) & (mark_lane == expert), 1.0, marks)
    xbuf[me_e, :, width:] = marks.astype(jnp.bfloat16)

    pending = []

    def remote(which, mask, source, target, to):
        return pltpu.make_async_remote_copy(
            src_ref=source,
            dst_ref=target,
            send_sem=ag_send.at[which, mask],
            recv_sem=ag_recv.at[which, to],
            device_id=device(flip(me_e, mask, bits), me_t),
            device_id_type=pl.DeviceIdType.MESH,
        )

    def share(which, buf):
        for mask in far_first:
            copy = remote(which, mask, buf.at[me_e], buf.at[me_e], me_e)
            copy.start()
            pending.append(copy)

    def arrive(which, buf, mask):
        e = flip(me_e, mask, bits)
        remote(which, mask, buf.at[e], buf.at[e], e).wait_recv()

    @pl.when(me_t == 1)
    def _():
        pl.semaphore_wait(barrier, ep_count - 1)
        tell(ready.at[1], sibling)

    @pl.when(me_t == 0)
    def _():
        pl.semaphore_wait(ready.at[1], 1)

    share(1, hbuf)
    share(0, xbuf)
    wo_copy.wait()
    pair_copies[0].wait_recv()
    for mask in reversed(far_first):
        arrive(1, hbuf, mask)

    flat_heads = hbuf[...].reshape(total_rows, hbuf.shape[2])
    cbuf[me_e] = jnp.concatenate(
        [jnp.dot(flat_heads, wo[t], preferred_element_type=jnp.float32) for t in range(2)], axis=1
    ).astype(jnp.bfloat16)
    share(2, cbuf)
    for mask in reversed(far_first):
        arrive(0, xbuf, mask)
    for copy in gain_copies + [router_copy] + expert_copies:
        copy.wait()
    for copy in pair_copies[1:]:
        copy.wait_recv()
    for mask in reversed(far_first):
        arrive(2, cbuf, mask)

    gains = [ref[...].astype(jnp.float32).reshape(1, width) for ref in (gm, gf, go)]
    mixed = jnp.concatenate([cbuf[o] for o in range(ep_count)], axis=1).astype(jnp.float32)
    stage = xbuf[...].reshape(total_rows, xbuf.shape[2])
    after_mix = (stage[:, :width].astype(jnp.float32) + gains[0] * normalize(mixed)).astype(
        jnp.bfloat16
    )
    mix_rows[...] = after_mix.reshape(mix_rows.shape)
    ffn_in = (normalize(after_mix.astype(jnp.float32)) * gains[1]).astype(jnp.bfloat16)
    norm_rows[...] = ffn_in.reshape(norm_rows.shape)
    affinity = jax.nn.sigmoid(
        lax.dot_general(
            ffn_in, router[...], (((1,), (1,)), ((), ())), preferred_element_type=jnp.float32
        )
    )
    hot = stage[:, width : width + affinity.shape[1]].astype(jnp.float32)
    chosen = affinity * hot
    lane = lax.broadcasted_iota(jnp.int32, chosen.shape, 1)
    whole = jnp.sum(chosen, axis=1, keepdims=True)
    outcome = jnp.zeros((total_rows, width), jnp.float32)
    for t in range(2):
        mine = jnp.sum(jnp.where(lane == me_e * 2 + t, chosen, 0.0), axis=1, keepdims=True)
        mine = mine / whole * routed_scale
        expert_out = swiglu(ffn_in, eg[t], eu[t], ed[t])
        outcome = outcome + expert_out.astype(jnp.float32) * mine
    terms[...] = outcome.astype(jnp.bfloat16).reshape(terms.shape)
    for mask in far_first:
        copy = remote(3, mask, terms.at[flip(me_e, mask, bits)], back.at[me_e], me_e)
        copy.start()
        pending.append(copy)
    for copy in shared_copies:
        copy.wait()
    combined = terms[me_e].astype(jnp.float32) + swiglu(
        norm_rows[me_e], sg[...], su[...], sd[...]
    ).astype(jnp.float32)
    for mask in reversed(far_first):
        arrive(3, back, mask)
        combined = combined + back[flip(me_e, mask, bits)].astype(jnp.float32)
    out_ref[...] = (
        mix_rows[me_e].astype(jnp.float32) + gains[2] * normalize(combined)
    ).astype(jnp.bfloat16)
    for copy in pending + pair_copies:
        copy.wait_send()


def local_fused(
    hidden_in,
    query_nope,
    query_rope,
    new_latent,
    new_rope,
    cache_latent,
    cache_rope,
    lengths,
    absorb_key,
    value_up,
    out_proj,
    gain_mix,
    gain_ffn_in,
    router,
    routes,
    expert_gate,
    expert_up,
    expert_down,
    shared_gate,
    shared_up,
    shared_down,
    gain_ffn_out,
):
    seq_count, width = hidden_in.shape
    heads, latent = query_nope.shape[1], cache_latent.shape[2]
    context, rope = cache_rope.shape[1:]
    ep_count = lax.axis_size("ep")
    bf = jnp.bfloat16
    score_scale = (query_nope.shape[-1] + query_rope.shape[-1]) ** (-0.5)
    dma = pltpu.SemaphoreType.DMA
    total_rows = ep_count * seq_count
    rows = seq_count * heads
    depth = seq_count * (latent + rope)
    rope_rows = jnp.swapaxes(cache_rope, 1, 2).reshape(seq_count * rope, context)
    router_rows = jnp.swapaxes(router, 0, 1)
    absorb_rows = jnp.transpose(absorb_key, (1, 2, 0)).reshape(-1, latent)
    route_rows = jnp.swapaxes(routes, 0, 1)
    gate, up, down = expert_gate[0], expert_up[0], expert_down[0]
    operands = (
        hidden_in,
        query_nope,
        query_rope,
        new_latent,
        new_rope,
        lengths,
        route_rows,
        gain_mix,
        gain_ffn_in,
        gain_ffn_out,
        absorb_rows,
        cache_latent,
        rope_rows,
        value_up,
        out_proj,
        router_rows,
        gate,
        up,
        down,
        shared_gate,
        shared_up,
        shared_down,
    )

    def near(array, lead=()):
        return pltpu.VMEM(lead + array.shape, array.dtype)

    flops = 2 * total_rows * width * out_proj.shape[1]
    return pl.pallas_call(
        functools.partial(fused_kernel, ep_count, score_scale),
        out_shape=pltpu.VMEM((seq_count, width), bf),
        in_specs=[pl.BlockSpec(memory_space=pl.ANY)] * len(operands),
        out_specs=pl.BlockSpec(memory_space=pltpu.VMEM),
        scratch_shapes=[near(a) for a in operands[:5]]
        + [pltpu.SMEM(lengths.shape, jnp.int32), pltpu.SMEM(route_rows.shape, jnp.int32)]
        + [near(a) for a in operands[7:11]]
        + [
            pltpu.VMEM((context, depth), bf),
            near(rope_rows),
            near(value_up),
            near(out_proj, (2,)),
            near(router_rows),
            near(gate, (2,)),
            near(up, (2,)),
            near(down, (2,)),
            near(shared_gate),
            near(shared_up),
            near(shared_down),
            pltpu.VMEM((latent, heads * value_up.shape[2]), bf),
            pltpu.VMEM((depth, rows), bf),
            pltpu.VMEM((8, depth), jnp.float32),
            pltpu.VMEM((rows, latent), bf),
            pltpu.VMEM((ep_count, seq_count, width + 128), bf),
            pltpu.VMEM((ep_count, seq_count, out_proj.shape[0]), bf),
            pltpu.VMEM((ep_count, total_rows, 2 * out_proj.shape[1]), bf),
            pltpu.VMEM((ep_count, seq_count, width), bf),
            pltpu.VMEM((ep_count, seq_count, width), bf),
            pltpu.VMEM((ep_count, seq_count, width), bf),
            pltpu.VMEM((ep_count, seq_count, width), bf),
            dma((len(operands),)),
            dma((seq_count,)),
            dma((4,)),
            dma((4,)),
            dma((4, ep_count)),
            dma((4, ep_count)),
            pltpu.SemaphoreType.REGULAR((2,)),
            pltpu.VMEM((context, rows), jnp.float32),
            pltpu.VMEM((rows, context), bf),
        ],
        compiler_params=pltpu.CompilerParams(
            collective_id=0, has_side_effects=True, vmem_limit_bytes=56 * 2**20
        ),
        cost_estimate=pl.CostEstimate(flops=flops, bytes_accessed=2**24, transcendentals=0),
        name="layer_step",
    )(*operands)


def local(*args):
    hidden_in, out_proj, router = args[0], args[10], args[13]
    device_count = lax.axis_size("ep") * lax.axis_size("tp")
    ep_count = lax.axis_size("ep")
    fits = (
        lax.axis_size("tp") == 2
        and ep_count & (ep_count - 1) == 0
        and hidden_in.shape[0] == 8
        and args[1].shape[1] == 16
        and device_count * hidden_in.shape[0] <= 256
        and out_proj.shape[1] % 128 == 0
        and router.shape[1] == device_count
    )
    return local_fused(*args) if fits else local_wide(*args)


def solution(mesh):
    placed = (
        P(("grp", "ep", "tp"), None),
        P(("grp", "ep", "tp"), None, None),
        P(("grp", "ep", "tp"), None, None),
        P(("grp", "ep", "tp"), None),
        P(("grp", "ep", "tp"), None),
        P(("grp", "ep", "tp"), None, None),
        P(("grp", "ep", "tp"), None, None),
        P(("grp", "ep", "tp")),
        P(),
        P(),
        P(None, ("ep", "tp")),
        P(),
        P(),
        P(),
        P(("grp", "ep"), None),
        P(("ep", "tp"), None, None),
        P(("ep", "tp"), None, None),
        P(("ep", "tp"), None, None),
        P(),
        P(),
        P(),
        P(),
    )
    return jax.shard_map(
        local, mesh=mesh, in_specs=placed, out_specs=P(("grp", "ep", "tp"), None), check_vma=False
    )
```

```python
import functools
import math

import jax
import jax.numpy as jnp
from jax import lax
from jax.experimental import pallas as pl
from jax.experimental.pallas import tpu as pltpu
from jax.sharding import PartitionSpec as P

ABLK = 512


rope_theta = 10000.0
norm_eps = 1e-06
routed_scale = 2.5
masked_score = -1e30


def normalize(values):
    return values * lax.rsqrt(jnp.mean(values * values, axis=-1, keepdims=True) + norm_eps)


def rotate(values, positions):
    half_dim = values.shape[-1] // 2
    inverse = rope_theta ** (-jnp.arange(half_dim, dtype=jnp.float32) * 2.0 / values.shape[-1])
    angles = positions * inverse
    cosine = jnp.cos(angles)
    sine_table = jnp.sin(angles)
    first_half = values[..., :half_dim]
    second_half = values[..., half_dim:]
    return jnp.concatenate(
        [
            first_half * cosine - second_half * sine_table,
            first_half * sine_table + second_half * cosine,
        ],
        axis=-1,
    )


def swiglu(flat_rows, gate_w, up_w, down_w):
    gate_part = jnp.dot(flat_rows, gate_w, preferred_element_type=jnp.float32)
    up_part = jnp.dot(flat_rows, up_w, preferred_element_type=jnp.float32)
    inner_rows = (jax.nn.silu(gate_part) * up_part).astype(jnp.bfloat16)
    return jnp.dot(inner_rows, down_w, preferred_element_type=jnp.float32).astype(jnp.bfloat16)


def local_wide(
    hidden_in,
    query_nope,
    query_rope,
    new_latent,
    new_rope,
    cache_latent,
    cache_rope,
    lengths,
    absorb_key,
    value_up,
    out_proj,
    gain_mix,
    gain_ffn_in,
    router,
    routes,
    expert_gate,
    expert_up,
    expert_down,
    shared_gate,
    shared_up,
    shared_down,
    gain_ffn_out,
):
    seq_count = hidden_in.shape[0]
    positions = lengths.astype(jnp.float32)
    query_latent = jnp.einsum(
        "shn,chn->shc", query_nope, absorb_key, preferred_element_type=jnp.float32
    ).astype(jnp.bfloat16)
    query_pe = rotate(query_rope.astype(jnp.float32), positions[:, None, None]).astype(jnp.bfloat16)
    latent_new = normalize(new_latent.astype(jnp.float32)).astype(jnp.bfloat16)
    key_new = rotate(new_rope.astype(jnp.float32), positions[:, None]).astype(jnp.bfloat16)
    score_scale = (query_nope.shape[-1] + query_rope.shape[-1]) ** (-0.5)
    new_score = (
        jnp.einsum("shc,sc->sh", query_latent, latent_new, preferred_element_type=jnp.float32)
        + jnp.einsum("shr,sr->sh", query_pe, key_new, preferred_element_type=jnp.float32)
    ) * score_scale

    def attend_block(block_index, loop_state):
        running_max, weight_total, weighted_sum = loop_state
        block_start = block_index * ABLK
        block_latent = lax.dynamic_slice_in_dim(cache_latent, block_start, ABLK, 1)
        block_rope = lax.dynamic_slice_in_dim(cache_rope, block_start, ABLK, 1)
        scores = (
            jnp.einsum(
                "shc,skc->shk", query_latent, block_latent, preferred_element_type=jnp.float32
            )
            + jnp.einsum("shr,skr->shk", query_pe, block_rope, preferred_element_type=jnp.float32)
        ) * score_scale
        key_index = block_start + lax.iota(jnp.int32, ABLK)
        in_range = key_index[None, None, :] < lengths[:, None, None]
        scores = jnp.where(in_range, scores, masked_score)
        new_max = jnp.maximum(running_max, jnp.max(scores, axis=-1))
        rescale = jnp.exp(running_max - new_max)
        weights = jnp.exp(scores - new_max[..., None])
        weight_total = weight_total * rescale + jnp.sum(weights, axis=-1)
        weighted_sum = weighted_sum * rescale[..., None] + jnp.einsum(
            "shk,skc->shc",
            weights.astype(jnp.bfloat16),
            block_latent,
            preferred_element_type=jnp.float32,
        )
        return (new_max, weight_total, weighted_sum)

    longest = jnp.max(lengths)
    block_count = (longest + ABLK - 1) // ABLK
    ones_start = jnp.ones_like(new_score)
    sum_start = ones_start[..., None] * latent_new.astype(jnp.float32)[:, None, :]
    final_max, weight_total, weighted_sum = lax.fori_loop(
        0, block_count, attend_block, (new_score, ones_start, sum_start)
    )
    latent_out = (weighted_sum / weight_total[..., None]).astype(jnp.bfloat16)
    heads_out = (
        jnp.einsum("shc,chv->shv", latent_out, value_up, preferred_element_type=jnp.float32)
        .astype(jnp.bfloat16)
        .reshape(seq_count, -1)
    )
    column_rows = jnp.dot(
        lax.all_gather(heads_out, ("ep", "tp"), axis=0, tiled=True),
        out_proj,
        preferred_element_type=jnp.float32,
    ).astype(jnp.bfloat16)
    mixed_rows = lax.all_to_all(column_rows, ("ep", "tp"), split_axis=0, concat_axis=1, tiled=True)
    after_mix = (
        hidden_in.astype(jnp.float32)
        + gain_mix.astype(jnp.float32) * normalize(mixed_rows.astype(jnp.float32))
    ).astype(jnp.bfloat16)
    ffn_in = (normalize(after_mix.astype(jnp.float32)) * gain_ffn_in.astype(jnp.float32)).astype(
        jnp.bfloat16
    )
    affinity = jax.nn.sigmoid(jnp.dot(ffn_in, router, preferred_element_type=jnp.float32))
    experts_total = router.shape[1]
    own_start = lax.axis_index("tp") * seq_count
    own_routes = lax.dynamic_slice_in_dim(routes, own_start, seq_count, 0)
    choose = own_routes[..., None] == lax.iota(jnp.int32, experts_total)[None, None, :]
    chosen = jnp.sum(jnp.where(choose, affinity[:, None, :], 0.0), axis=-1)
    route_weights = chosen / jnp.sum(chosen, axis=-1, keepdims=True) * routed_scale
    group_rows, top_count = routes.shape
    capacity = 2 * ((group_rows * top_count + experts_total - 1) // experts_total)
    flat_routes = routes.reshape(-1)
    order_index = lax.iota(jnp.int32, group_rows * top_count)
    same_expert = flat_routes[:, None] == flat_routes[None, :]
    earlier = order_index[None, :] < order_index[:, None]
    slot_number = jnp.sum(jnp.logical_and(same_expert, earlier), axis=1)
    slot_number = slot_number.reshape(group_rows, top_count)
    own_slots = lax.dynamic_slice_in_dim(slot_number, own_start, seq_count, 0)
    slot_index = own_routes * capacity + own_slots
    slots_total = experts_total * capacity
    slot_table = jnp.any(
        slot_index[None, :, :] == lax.iota(jnp.int32, slots_total)[:, None, None], axis=-1
    ).astype(jnp.bfloat16)
    outgoing_terms = jnp.dot(slot_table, ffn_in, preferred_element_type=jnp.float32)
    outgoing = outgoing_terms.astype(jnp.bfloat16).reshape(experts_total, capacity, -1)
    received = lax.all_to_all(outgoing, ("ep", "tp"), split_axis=0, concat_axis=0, tiled=True)
    ep_count = lax.axis_size("ep")
    tp_count = lax.axis_size("tp")
    item_count = received.shape[1]
    width = received.shape[2]
    merged = jnp.sum(received.reshape(ep_count, tp_count, item_count, width), axis=1)
    outputs = swiglu(
        merged.reshape(ep_count * item_count, width), expert_gate[0], expert_up[0], expert_down[0]
    )
    copies = jnp.broadcast_to(
        outputs.reshape(ep_count, 1, item_count, width), (ep_count, tp_count, item_count, width)
    )
    copies = copies.reshape(ep_count * tp_count, item_count, width)
    returned = lax.all_to_all(copies, ("ep", "tp"), split_axis=0, concat_axis=0, tiled=True)
    picked = returned.reshape(slots_total, -1)[slot_index]
    routed = jnp.sum(picked.astype(jnp.float32) * route_weights[..., None], axis=1)
    shared = swiglu(ffn_in, shared_gate, shared_up, shared_down)
    combined = routed + shared.astype(jnp.float32)
    return (
        after_mix.astype(jnp.float32) + gain_ffn_out.astype(jnp.float32) * normalize(combined)
    ).astype(jnp.bfloat16)


def flip(index, mask, bits):
    result = 0
    for b in range(bits):
        bit = (index // 2**b) % 2
        result = result + (1 - bit if mask >> b & 1 else bit) * 2**b
    return result


def fused_kernel(
    ep_count,
    score_scale,
    hidden_hbm,
    qn_hbm,
    qr_hbm,
    nl_hbm,
    nr_hbm,
    len_hbm,
    routes_hbm,
    gm_hbm,
    gf_hbm,
    go_hbm,
    ab_hbm,
    cl_hbm,
    cr_hbm,
    vup_hbm,
    wo_hbm,
    router_hbm,
    eg_hbm,
    eu_hbm,
    ed_hbm,
    sg_hbm,
    su_hbm,
    sd_hbm,
    out_ref,
    hidden,
    qn,
    qr,
    nl,
    nr,
    length_of,
    route_of,
    gm,
    gf,
    go,
    ab,
    keys,
    rope_keys,
    vraw,
    wo,
    router,
    egu,
    ed,
    sgu,
    sd,
    vup,
    wq,
    new_keys,
    scores,
    turned_weights,
    lat,
    xbuf,
    hbuf,
    cbuf,
    norm_rows,
    mix_rows,
    terms,
    back,
    local_sem,
    pair_send,
    pair_recv,
    far_send,
    far_recv,
    ready,
):
    seq_count, heads, nope = qn.shape
    rope = qr.shape[2]
    width = out_ref.shape[1]
    latent = nl.shape[1]
    rows = seq_count * heads
    chunks, _, unit, _ = hbuf.shape
    chunk_rows = ep_count * unit
    chunk_depth = unit * (latent + rope)
    bits = (ep_count - 1).bit_length()
    me_e = lax.axis_index("ep")
    me_t = lax.axis_index("tp")

    def device(e, t):
        return {"ep": e, "tp": t}

    sibling = device(me_e, 1 - me_t)
    far_first = list(range(ep_count - 1, 0, -1))
    barrier = pltpu.get_barrier_semaphore()

    def tell(semaphore, target):
        pl.semaphore_signal(
            semaphore, inc=1, device_id=target, device_id_type=pl.DeviceIdType.MESH
        )

    @pl.when(me_t == 1)
    def _():
        tell(barrier, sibling)

    sems = iter(range(local_sem.shape[0]))

    def fetch(source, target, sem=None):
        copy = pltpu.make_async_copy(source, target, local_sem.at[next(sems) if sem is None else sem])
        copy.start()
        return copy

    def all_of(region, sem):
        return pltpu.make_async_copy(region, region, local_sem.at[sem])

    len_copy = fetch(len_hbm, length_of)
    query_copies = [
        fetch(s, t) for s, t in ((qr_hbm, qr), (nl_hbm, nl), (nr_hbm, nr), (qn_hbm, qn))
    ]
    absorb_copy = fetch(ab_hbm, ab)
    value_copy = fetch(vup_hbm, vraw)
    row_copies = [fetch(routes_hbm, route_of), fetch(hidden_hbm, hidden)]
    rope_copy = fetch(cr_hbm, rope_keys)
    cache_copies = []
    for c in range(chunks):
        sem = next(sems)
        for i in range(unit):
            at = c * chunk_depth + i * latent
            fetch(cl_hbm.at[c * unit + i], keys.at[:, at : at + latent], sem)
        at = c * chunk_depth
        cache_copies.append(all_of(keys.at[:, at : at + unit * latent], sem))

    def to_sibling(index, source, target):
        return pltpu.make_async_remote_copy(
            src_ref=source,
            dst_ref=target,
            send_sem=pair_send.at[index],
            recv_sem=pair_recv.at[index],
            device_id=sibling,
            device_id_type=pl.DeviceIdType.MESH,
        )

    pair_copies = [
        to_sibling(index, source, target)
        for index, (source, target) in enumerate(
            (
                (wo_hbm, wo.at[me_t]),
                (eg_hbm, egu.at[me_t, 0]),
                (eu_hbm, egu.at[me_t, 1]),
                (ed_hbm, ed.at[me_t]),
            )
        )
    ]

    @pl.when(me_t == 0)
    def _():
        pl.semaphore_wait(barrier, 1)
        tell(ready.at[0], sibling)

    @pl.when(me_t == 1)
    def _():
        pl.semaphore_wait(ready.at[0], 1)
        for mask in far_first:
            tell(barrier, device(flip(me_e, mask, bits), me_t))

    for copy in pair_copies:
        copy.start()

    value_dim = vraw.shape[2]
    step = 256 // heads
    order_row = lax.broadcasted_iota(jnp.int32, (256, 256), 0)
    order_lane = lax.broadcasted_iota(jnp.int32, (256, 256), 1)
    order = jnp.where(
        order_lane == order_row % step * heads + order_row // step, 1.0, 0.0
    ).astype(jnp.bfloat16)

    half = rope // 2
    turn_row = lax.broadcasted_iota(jnp.int32, (seq_count, rope), 0)
    turn_lane = lax.broadcasted_iota(jnp.int32, (seq_count, rope), 1)
    inverse = jnp.zeros((seq_count, rope), jnp.float32)
    for i in range(half):
        inverse = jnp.where(turn_lane % half == i, rope_theta ** (-2.0 * i / rope), inverse)
    len_copy.wait()
    position = jnp.zeros((seq_count, rope), jnp.float32)
    for s in range(seq_count):
        position = jnp.where(turn_row == s, length_of[s].astype(jnp.float32), position)
    angles = position * inverse
    cosine = jnp.cos(angles)
    sine = jnp.sin(angles) * jnp.where(turn_lane < half, -1.0, 1.0)

    def turned(values, cos_rows, sin_rows):
        swapped = jnp.concatenate([values[:, half:], values[:, :half]], axis=1)
        return values * cos_rows + swapped * sin_rows

    def per_head(table):
        return jnp.broadcast_to(table[:, None, :], (seq_count, heads, rope)).reshape(rows, rope)

    for copy in query_copies:
        copy.wait()
    query_rows = qr[...].astype(jnp.float32).reshape(rows, rope)
    q_pe = turned(query_rows, per_head(cosine), per_head(sine))
    key_rows = turned(nr[...].astype(jnp.float32), cosine, sine)
    new_rows = normalize(nl[...].astype(jnp.float32)).astype(jnp.bfloat16).astype(jnp.float32)

    def places(s):
        base = s // unit * chunk_depth
        at = base + s % unit * latent
        rope_at = base + unit * latent + s % unit * rope
        return slice(at, at + latent), slice(rope_at, rope_at + rope)

    new_keys[...] = jnp.zeros_like(new_keys)
    for s in range(seq_count):
        new_keys[0:1, places(s)[0]] = new_rows[s : s + 1, :]
    for c in range(chunks):
        at = c * chunk_depth + unit * latent
        new_keys[0:1, at : at + unit * rope] = jnp.concatenate(
            [key_rows[s : s + 1, :] for s in range(c * unit, (c + 1) * unit)], axis=1
        )

    nope_rows = qn[...].astype(jnp.float32).reshape(rows, nope)
    row_head = lax.broadcasted_iota(jnp.int32, (rows, 2 * nope), 0) % heads
    pair_lane = lax.broadcasted_iota(jnp.int32, (rows, 2 * nope), 1) // nope
    doubled = jnp.concatenate([nope_rows, nope_rows], axis=1)
    spread_query = jnp.concatenate(
        [
            jnp.where(row_head == pair_lane + 2 * j, doubled, 0.0).astype(jnp.bfloat16)
            for j in range(heads // 2)
        ],
        axis=1,
    )
    absorb_copy.wait()
    q_lat = jnp.dot(spread_query, ab[...], preferred_element_type=jnp.float32)
    q_turned = q_lat.T
    lane_seq = lax.broadcasted_iota(jnp.int32, (latent, rows), 1) // heads
    rope_turned = jnp.concatenate([q_pe] * (128 // rope), axis=1).T[:rope]
    rope_seq = lax.broadcasted_iota(jnp.int32, (rope, rows), 1) // heads
    for s in range(seq_count):
        place, rope_place = places(s)
        wq[place, :] = jnp.where(lane_seq == s, q_turned, 0.0).astype(jnp.bfloat16)
        wq[rope_place, :] = jnp.where(rope_seq == s, rope_turned, 0.0).astype(jnp.bfloat16)

    value_copy.wait()
    for b in range(0, latent // step, 2):
        blocks = [
            vraw[i * step : (i + 1) * step].reshape(step * heads, value_dim) for i in (b, b + 1)
        ]
        ordered = jnp.dot(
            order, jnp.concatenate(blocks, axis=1), preferred_element_type=jnp.float32
        ).astype(jnp.bfloat16)
        for i in range(2):
            for h in range(heads):
                vup[(b + i) * step : (b + i + 1) * step, h * value_dim : (h + 1) * value_dim] = (
                    ordered[h * step : (h + 1) * step, i * value_dim : (i + 1) * value_dim]
                )

    for copy in row_copies:
        copy.wait()
    mark_shape = (seq_count, xbuf.shape[3] - width)
    mark_row = lax.broadcasted_iota(jnp.int32, mark_shape, 0)
    mark_lane = lax.broadcasted_iota(jnp.int32, mark_shape, 1)
    marks = jnp.zeros(mark_shape, jnp.float32)
    for s in range(seq_count):
        for j in range(route_of.shape[0]):
            expert = route_of[j, me_t * seq_count + s]
            marks = jnp.where((mark_row == s) & (mark_lane == expert), 1.0, marks)
    own_rows = hidden[...].astype(jnp.float32)
    for c in range(chunks):
        part = slice(c * unit, (c + 1) * unit)
        xbuf[me_e, c, :, 0:width] = own_rows[part].astype(jnp.bfloat16)
        xbuf[me_e, c, :, width:] = marks[part].astype(jnp.bfloat16)

    context = keys.shape[0]
    lengths_row = jnp.zeros((1, rows), jnp.int32)
    lane_of = lax.broadcasted_iota(jnp.int32, (1, rows), 1) // heads
    for s in range(seq_count):
        lengths_row = jnp.where(lane_of == s, length_of[s], lengths_row)
    new_score = jnp.dot(
        new_keys[...].astype(jnp.bfloat16), wq[...], preferred_element_type=jnp.float32
    )[0:1]
    rope_copy.wait()
    for c in range(chunks):
        at = c * chunk_depth + unit * latent
        keys[:, at : at + unit * rope] = rope_keys[c * unit * rope : (c + 1) * unit * rope].T

    block = 256
    key_index = lax.broadcasted_iota(jnp.int32, (block, rows), 0)
    power = score_scale * math.log2(math.e)

    def attend(c):
        deep = slice(c * chunk_depth, (c + 1) * chunk_depth)
        query = wq[deep, :]
        tops = jnp.full((8, rows), masked_score, jnp.float32)
        for k in range(0, context, block):
            found = jnp.dot(keys[k : k + block, deep], query, preferred_element_type=jnp.float32)
            found = jnp.where(key_index < lengths_row - k, found, masked_score)
            scores[k : k + block, :] = found
            tops = jnp.maximum(tops, jnp.max(found.reshape(block // 8, 8, rows), axis=0))
        row_max = jnp.maximum(jnp.max(tops, axis=0, keepdims=True), new_score)
        sums = jnp.zeros((8, rows), jnp.float32)
        for k in range(0, context, block):
            weights = jnp.exp2((scores[k : k + block, :] - row_max) * power)
            sums = sums + jnp.sum(weights.reshape(block // 8, 8, rows), axis=0)
            turned_weights[:, k : k + block] = weights.astype(jnp.bfloat16).T
        new_weight = jnp.exp2((new_score - row_max) * power)
        weight_total = jnp.sum(sums, axis=0, keepdims=True) + new_weight
        new_weight = new_weight.astype(jnp.bfloat16).astype(jnp.float32)
        side = jnp.concatenate(
            [weight_total, new_weight, jnp.zeros((6, rows), jnp.float32)], axis=0
        ).T
        for s in range(c * unit, (c + 1) * unit):
            part = slice(s * heads, (s + 1) * heads)
            weighted = jnp.dot(
                turned_weights[part, :], keys[:, places(s)[0]], preferred_element_type=jnp.float32
            )
            weighted = weighted + side[part, 1:2] * new_rows[s : s + 1, :]
            lat[part, :] = (weighted / side[part, 0:1]).astype(jnp.bfloat16)
        spread = jnp.dot(
            lat[c * unit * heads : (c + 1) * unit * heads, :],
            vup[...],
            preferred_element_type=jnp.float32,
        )
        own_heads = []
        head_row = lax.broadcasted_iota(jnp.int32, (unit, heads, value_dim), 1)
        for h in range(heads):
            piece = spread[:, h * value_dim : (h + 1) * value_dim].reshape(unit, heads, value_dim)
            own_heads.append(jnp.sum(jnp.where(head_row == h, piece, 0.0), axis=1))
        hbuf[c, me_e] = jnp.concatenate(own_heads, axis=1).astype(jnp.bfloat16)

    def remote(group, mask, source, target):
        return pltpu.make_async_remote_copy(
            src_ref=source,
            dst_ref=target,
            send_sem=far_send.at[group],
            recv_sem=far_recv.at[group],
            device_id=device(flip(me_e, mask, bits), me_t),
            device_id_type=pl.DeviceIdType.MESH,
        )

    def share(group, slot):
        for mask in far_first:
            remote(group, mask, slot, slot).start()

    peers = pl.ds(0, ep_count - 1)
    drains = []

    def gathered(group, region):
        whole = remote(group, 1, region, region)
        drains.append(whole)
        whole.wait_recv()

    def columns(c):
        flat_heads = hbuf[c].reshape(chunk_rows, hbuf.shape[3])
        cbuf[c, me_e] = jnp.concatenate(
            [
                jnp.dot(flat_heads, wo[t], preferred_element_type=jnp.float32)
                for t in range(wo.shape[0])
            ],
            axis=1,
        ).astype(jnp.bfloat16)
        share(2 + c, cbuf.at[c, me_e])

    def experts(c):
        mixed = jnp.concatenate([cbuf[c, o] for o in range(ep_count)], axis=1).astype(jnp.float32)
        stage = xbuf[:, c].reshape(chunk_rows, xbuf.shape[3])
        after_mix = (stage[:, :width].astype(jnp.float32) + gains[0] * normalize(mixed)).astype(
            jnp.bfloat16
        )
        mix_rows[c] = after_mix.reshape(ep_count, unit, width)
        ffn_in = (normalize(after_mix.astype(jnp.float32)) * gains[1]).astype(jnp.bfloat16)
        norm_rows[c] = ffn_in.reshape(ep_count, unit, width)
        affinity = jax.nn.sigmoid(
            lax.dot_general(
                ffn_in, router[...], (((1,), (1,)), ((), ())), preferred_element_type=jnp.float32
            )
        )
        hot = stage[:, width : width + affinity.shape[1]].astype(jnp.float32)
        chosen = affinity * hot
        lane = lax.broadcasted_iota(jnp.int32, chosen.shape, 1)
        whole = jnp.sum(chosen, axis=1, keepdims=True)
        outcome = jnp.zeros((chunk_rows, width), jnp.float32)
        for t in range(ed.shape[0]):
            mine = jnp.sum(jnp.where(lane == me_e * 2 + t, chosen, 0.0), axis=1, keepdims=True)
            mine = mine / whole * routed_scale
            expert_out = swiglu(ffn_in, egu[t, 0], egu[t, 1], ed[t])
            outcome = outcome + expert_out.astype(jnp.float32) * mine
        terms[c] = outcome.astype(jnp.bfloat16).reshape(ep_count, unit, width)
        for mask in far_first:
            remote(4 + c, mask, terms.at[c, flip(me_e, mask, bits)], back.at[c, me_e]).start()
        back[c, me_e] = terms[c, me_e]

    for copy in cache_copies[:1]:
        copy.wait()
    attend(0)

    @pl.when(me_t == 1)
    def _():
        pl.semaphore_wait(barrier, ep_count - 1)
        tell(ready.at[1], sibling)

    @pl.when(me_t == 0)
    def _():
        pl.semaphore_wait(ready.at[1], 1)

    share(0, hbuf.at[0, me_e])
    cross = ep_count // 2
    remote(7, cross, xbuf.at[me_e], xbuf.at[me_e]).start()
    for mask in range(cross - 1, 0, -1):
        remote(6, mask, xbuf.at[me_e], xbuf.at[me_e]).start()

    cache_copies[1].wait()
    wo_copy = fetch(wo_hbm, wo.at[me_t])
    gain_copies = [fetch(s, t) for s, t in ((gm_hbm, gm), (gf_hbm, gf), (go_hbm, go))]
    router_copy = fetch(router_hbm, router)
    sem = next(sems)
    fetch(eg_hbm, egu.at[me_t, 0], sem)
    fetch(eu_hbm, egu.at[me_t, 1], sem)
    expert_copies = [all_of(egu.at[me_t], sem), fetch(ed_hbm, ed.at[me_t])]
    sem = next(sems)
    fetch(sg_hbm, sgu.at[0], sem)
    fetch(su_hbm, sgu.at[1], sem)
    shared_copies = [all_of(sgu, sem), fetch(sd_hbm, sd)]
    attend(1)
    share(1, hbuf.at[1, me_e])

    wo_copy.wait()
    pair_copies[0].wait_recv()
    gathered(0, hbuf.at[0, peers])
    other = flip(me_e, cross, bits)
    crossed = remote(7, cross, xbuf.at[other], xbuf.at[other])
    crossed.wait_recv()
    for mask in range(cross - 1, 0, -1):
        remote(6, mask, xbuf.at[other], xbuf.at[other]).start()
    columns(0)
    gathered(1, hbuf.at[1, peers])
    columns(1)
    for copy in gain_copies + [router_copy] + expert_copies:
        copy.wait()
    for copy in pair_copies[1:]:
        copy.wait_recv()
    gains = [ref[...].astype(jnp.float32).reshape(1, width) for ref in (gm, gf, go)]
    gathered(2, cbuf.at[0, peers])
    gathered(6, xbuf.at[pl.ds(0, ep_count - 2)])
    experts(0)
    gathered(3, cbuf.at[1, peers])
    experts(1)
    for copy in shared_copies:
        copy.wait()
    own_in = jnp.concatenate(
        [norm_rows[c, me_e].astype(jnp.float32) for c in range(chunks)], axis=0
    ).astype(jnp.bfloat16)
    combined = swiglu(own_in, sgu[0], sgu[1], sd[...]).astype(jnp.float32)
    returned = []
    for c in range(chunks):
        gathered(4 + c, back.at[c, peers])
        returned.append(jnp.sum(back[c].astype(jnp.float32), axis=0))
    combined = combined + jnp.concatenate(returned, axis=0)
    own_mix = jnp.concatenate(
        [mix_rows[c, me_e].astype(jnp.float32) for c in range(chunks)], axis=0
    )
    out_ref[...] = (own_mix + gains[2] * normalize(combined)).astype(jnp.bfloat16)
    for copy in pair_copies + [crossed] + drains:
        copy.wait_send()


def local_fused(
    hidden_in,
    query_nope,
    query_rope,
    new_latent,
    new_rope,
    cache_latent,
    cache_rope,
    lengths,
    absorb_key,
    value_up,
    out_proj,
    gain_mix,
    gain_ffn_in,
    router,
    routes,
    expert_gate,
    expert_up,
    expert_down,
    shared_gate,
    shared_up,
    shared_down,
    gain_ffn_out,
):
    seq_count, width = hidden_in.shape
    heads, latent = query_nope.shape[1], cache_latent.shape[2]
    context, rope = cache_rope.shape[1:]
    ep_count = lax.axis_size("ep")
    bf = jnp.bfloat16
    score_scale = (query_nope.shape[-1] + query_rope.shape[-1]) ** (-0.5)
    dma = pltpu.SemaphoreType.DMA
    chunks = 2
    unit = seq_count // chunks
    total_rows = ep_count * seq_count
    rows = seq_count * heads
    depth = seq_count * (latent + rope)
    rope_rows = jnp.swapaxes(cache_rope, 1, 2).reshape(seq_count * rope, context)
    router_rows = jnp.swapaxes(router, 0, 1)
    absorb_rows = jnp.transpose(absorb_key, (1, 2, 0)).reshape(-1, latent)
    route_rows = jnp.swapaxes(routes, 0, 1)
    gate, up, down = expert_gate[0], expert_up[0], expert_down[0]
    operands = (
        hidden_in,
        query_nope,
        query_rope,
        new_latent,
        new_rope,
        lengths,
        route_rows,
        gain_mix,
        gain_ffn_in,
        gain_ffn_out,
        absorb_rows,
        cache_latent,
        rope_rows,
        value_up,
        out_proj,
        router_rows,
        gate,
        up,
        down,
        shared_gate,
        shared_up,
        shared_down,
    )

    def near(array, lead=()):
        return pltpu.VMEM(lead + array.shape, array.dtype)

    flops = 2 * total_rows * width * out_proj.shape[1]
    return pl.pallas_call(
        functools.partial(fused_kernel, ep_count, score_scale),
        out_shape=pltpu.VMEM((seq_count, width), bf),
        in_specs=[pl.BlockSpec(memory_space=pl.ANY)] * len(operands),
        out_specs=pl.BlockSpec(memory_space=pltpu.VMEM),
        scratch_shapes=[near(a) for a in operands[:5]]
        + [pltpu.SMEM(lengths.shape, jnp.int32), pltpu.SMEM(route_rows.shape, jnp.int32)]
        + [near(a) for a in operands[7:11]]
        + [
            pltpu.VMEM((context, depth), bf),
            near(rope_rows),
            near(value_up),
            near(out_proj, (2,)),
            near(router_rows),
            near(gate, (2, 2)),
            near(down, (2,)),
            near(shared_gate, (2,)),
            near(shared_down),
            pltpu.VMEM((latent, heads * value_up.shape[2]), bf),
            pltpu.VMEM((depth, rows), bf),
            pltpu.VMEM((8, depth), jnp.float32),
            pltpu.VMEM((context, rows), jnp.float32),
            pltpu.VMEM((rows, context), bf),
            pltpu.VMEM((rows, latent), bf),
            pltpu.VMEM((ep_count, chunks, unit, width + 128), bf),
            pltpu.VMEM((chunks, ep_count, unit, out_proj.shape[0]), bf),
            pltpu.VMEM((chunks, ep_count, ep_count * unit, 2 * out_proj.shape[1]), bf),
            pltpu.VMEM((chunks, ep_count, unit, width), bf),
            pltpu.VMEM((chunks, ep_count, unit, width), bf),
            pltpu.VMEM((chunks, ep_count, unit, width), bf),
            pltpu.VMEM((chunks, ep_count, unit, width), bf),
            dma((21,)),
            dma((4,)),
            dma((4,)),
            dma((8,)),
            dma((8,)),
            pltpu.SemaphoreType.REGULAR((2,)),
        ],
        compiler_params=pltpu.CompilerParams(
            collective_id=0, has_side_effects=True, vmem_limit_bytes=56 * 2**20
        ),
        cost_estimate=pl.CostEstimate(flops=flops, bytes_accessed=2**24, transcendentals=0),
        name="layer_step",
    )(*operands)


def local(*args):
    hidden_in, out_proj, router = args[0], args[10], args[13]
    device_count = lax.axis_size("ep") * lax.axis_size("tp")
    ep_count = lax.axis_size("ep")
    fits = (
        lax.axis_size("tp") == 2
        and ep_count & (ep_count - 1) == 0
        and hidden_in.shape[0] == 8
        and args[1].shape[1] == 16
        and device_count * hidden_in.shape[0] <= 256
        and out_proj.shape[1] % 128 == 0
        and router.shape[1] == device_count
    )
    return local_fused(*args) if fits else local_wide(*args)


def solution(mesh):
    placed = (
        P(("grp", "ep", "tp"), None),
        P(("grp", "ep", "tp"), None, None),
        P(("grp", "ep", "tp"), None, None),
        P(("grp", "ep", "tp"), None),
        P(("grp", "ep", "tp"), None),
        P(("grp", "ep", "tp"), None, None),
        P(("grp", "ep", "tp"), None, None),
        P(("grp", "ep", "tp")),
        P(),
        P(),
        P(None, ("ep", "tp")),
        P(),
        P(),
        P(),
        P(("grp", "ep"), None),
        P(("ep", "tp"), None, None),
        P(("ep", "tp"), None, None),
        P(("ep", "tp"), None, None),
        P(),
        P(),
        P(),
        P(),
    )
    return jax.shard_map(
        local, mesh=mesh, in_specs=placed, out_specs=P(("grp", "ep", "tp"), None), check_vma=False
    )
```

```python
import functools
import math

import jax
import jax.numpy as jnp
from jax import lax
from jax.experimental import pallas as pl
from jax.experimental.pallas import tpu as pltpu
from jax.sharding import PartitionSpec as P

ABLK = 512


rope_theta = 10000.0
norm_eps = 1e-06
routed_scale = 2.5
masked_score = -1e30


def normalize(values):
    return values * lax.rsqrt(jnp.mean(values * values, axis=-1, keepdims=True) + norm_eps)


def rotate(values, positions):
    half_dim = values.shape[-1] // 2
    inverse = rope_theta ** (-jnp.arange(half_dim, dtype=jnp.float32) * 2.0 / values.shape[-1])
    angles = positions * inverse
    cosine = jnp.cos(angles)
    sine_table = jnp.sin(angles)
    first_half = values[..., :half_dim]
    second_half = values[..., half_dim:]
    return jnp.concatenate(
        [
            first_half * cosine - second_half * sine_table,
            first_half * sine_table + second_half * cosine,
        ],
        axis=-1,
    )


def swiglu(flat_rows, gate_w, up_w, down_w):
    gate_part = jnp.dot(flat_rows, gate_w, preferred_element_type=jnp.float32)
    up_part = jnp.dot(flat_rows, up_w, preferred_element_type=jnp.float32)
    inner_rows = (jax.nn.silu(gate_part) * up_part).astype(jnp.bfloat16)
    return jnp.dot(inner_rows, down_w, preferred_element_type=jnp.float32).astype(jnp.bfloat16)


def local_wide(
    hidden_in,
    query_nope,
    query_rope,
    new_latent,
    new_rope,
    cache_latent,
    cache_rope,
    lengths,
    absorb_key,
    value_up,
    out_proj,
    gain_mix,
    gain_ffn_in,
    router,
    routes,
    expert_gate,
    expert_up,
    expert_down,
    shared_gate,
    shared_up,
    shared_down,
    gain_ffn_out,
):
    seq_count = hidden_in.shape[0]
    positions = lengths.astype(jnp.float32)
    query_latent = jnp.einsum(
        "shn,chn->shc", query_nope, absorb_key, preferred_element_type=jnp.float32
    ).astype(jnp.bfloat16)
    query_pe = rotate(query_rope.astype(jnp.float32), positions[:, None, None]).astype(jnp.bfloat16)
    latent_new = normalize(new_latent.astype(jnp.float32)).astype(jnp.bfloat16)
    key_new = rotate(new_rope.astype(jnp.float32), positions[:, None]).astype(jnp.bfloat16)
    score_scale = (query_nope.shape[-1] + query_rope.shape[-1]) ** (-0.5)
    new_score = (
        jnp.einsum("shc,sc->sh", query_latent, latent_new, preferred_element_type=jnp.float32)
        + jnp.einsum("shr,sr->sh", query_pe, key_new, preferred_element_type=jnp.float32)
    ) * score_scale

    def attend_block(block_index, loop_state):
        running_max, weight_total, weighted_sum = loop_state
        block_start = block_index * ABLK
        block_latent = lax.dynamic_slice_in_dim(cache_latent, block_start, ABLK, 1)
        block_rope = lax.dynamic_slice_in_dim(cache_rope, block_start, ABLK, 1)
        scores = (
            jnp.einsum(
                "shc,skc->shk", query_latent, block_latent, preferred_element_type=jnp.float32
            )
            + jnp.einsum("shr,skr->shk", query_pe, block_rope, preferred_element_type=jnp.float32)
        ) * score_scale
        key_index = block_start + lax.iota(jnp.int32, ABLK)
        in_range = key_index[None, None, :] < lengths[:, None, None]
        scores = jnp.where(in_range, scores, masked_score)
        new_max = jnp.maximum(running_max, jnp.max(scores, axis=-1))
        rescale = jnp.exp(running_max - new_max)
        weights = jnp.exp(scores - new_max[..., None])
        weight_total = weight_total * rescale + jnp.sum(weights, axis=-1)
        weighted_sum = weighted_sum * rescale[..., None] + jnp.einsum(
            "shk,skc->shc",
            weights.astype(jnp.bfloat16),
            block_latent,
            preferred_element_type=jnp.float32,
        )
        return (new_max, weight_total, weighted_sum)

    longest = jnp.max(lengths)
    block_count = (longest + ABLK - 1) // ABLK
    ones_start = jnp.ones_like(new_score)
    sum_start = ones_start[..., None] * latent_new.astype(jnp.float32)[:, None, :]
    final_max, weight_total, weighted_sum = lax.fori_loop(
        0, block_count, attend_block, (new_score, ones_start, sum_start)
    )
    latent_out = (weighted_sum / weight_total[..., None]).astype(jnp.bfloat16)
    heads_out = (
        jnp.einsum("shc,chv->shv", latent_out, value_up, preferred_element_type=jnp.float32)
        .astype(jnp.bfloat16)
        .reshape(seq_count, -1)
    )
    column_rows = jnp.dot(
        lax.all_gather(heads_out, ("ep", "tp"), axis=0, tiled=True),
        out_proj,
        preferred_element_type=jnp.float32,
    ).astype(jnp.bfloat16)
    mixed_rows = lax.all_to_all(column_rows, ("ep", "tp"), split_axis=0, concat_axis=1, tiled=True)
    after_mix = (
        hidden_in.astype(jnp.float32)
        + gain_mix.astype(jnp.float32) * normalize(mixed_rows.astype(jnp.float32))
    ).astype(jnp.bfloat16)
    ffn_in = (normalize(after_mix.astype(jnp.float32)) * gain_ffn_in.astype(jnp.float32)).astype(
        jnp.bfloat16
    )
    affinity = jax.nn.sigmoid(jnp.dot(ffn_in, router, preferred_element_type=jnp.float32))
    experts_total = router.shape[1]
    own_start = lax.axis_index("tp") * seq_count
    own_routes = lax.dynamic_slice_in_dim(routes, own_start, seq_count, 0)
    choose = own_routes[..., None] == lax.iota(jnp.int32, experts_total)[None, None, :]
    chosen = jnp.sum(jnp.where(choose, affinity[:, None, :], 0.0), axis=-1)
    route_weights = chosen / jnp.sum(chosen, axis=-1, keepdims=True) * routed_scale
    group_rows, top_count = routes.shape
    capacity = 2 * ((group_rows * top_count + experts_total - 1) // experts_total)
    flat_routes = routes.reshape(-1)
    order_index = lax.iota(jnp.int32, group_rows * top_count)
    same_expert = flat_routes[:, None] == flat_routes[None, :]
    earlier = order_index[None, :] < order_index[:, None]
    slot_number = jnp.sum(jnp.logical_and(same_expert, earlier), axis=1)
    slot_number = slot_number.reshape(group_rows, top_count)
    own_slots = lax.dynamic_slice_in_dim(slot_number, own_start, seq_count, 0)
    slot_index = own_routes * capacity + own_slots
    slots_total = experts_total * capacity
    slot_table = jnp.any(
        slot_index[None, :, :] == lax.iota(jnp.int32, slots_total)[:, None, None], axis=-1
    ).astype(jnp.bfloat16)
    outgoing_terms = jnp.dot(slot_table, ffn_in, preferred_element_type=jnp.float32)
    outgoing = outgoing_terms.astype(jnp.bfloat16).reshape(experts_total, capacity, -1)
    received = lax.all_to_all(outgoing, ("ep", "tp"), split_axis=0, concat_axis=0, tiled=True)
    ep_count = lax.axis_size("ep")
    tp_count = lax.axis_size("tp")
    item_count = received.shape[1]
    width = received.shape[2]
    merged = jnp.sum(received.reshape(ep_count, tp_count, item_count, width), axis=1)
    outputs = swiglu(
        merged.reshape(ep_count * item_count, width), expert_gate[0], expert_up[0], expert_down[0]
    )
    copies = jnp.broadcast_to(
        outputs.reshape(ep_count, 1, item_count, width), (ep_count, tp_count, item_count, width)
    )
    copies = copies.reshape(ep_count * tp_count, item_count, width)
    returned = lax.all_to_all(copies, ("ep", "tp"), split_axis=0, concat_axis=0, tiled=True)
    picked = returned.reshape(slots_total, -1)[slot_index]
    routed = jnp.sum(picked.astype(jnp.float32) * route_weights[..., None], axis=1)
    shared = swiglu(ffn_in, shared_gate, shared_up, shared_down)
    combined = routed + shared.astype(jnp.float32)
    return (
        after_mix.astype(jnp.float32) + gain_ffn_out.astype(jnp.float32) * normalize(combined)
    ).astype(jnp.bfloat16)


def flip(index, mask, bits):
    result = 0
    for b in range(bits):
        bit = (index // 2**b) % 2
        result = result + (1 - bit if mask >> b & 1 else bit) * 2**b
    return result


def fused_kernel(
    ep_count,
    score_scale,
    hidden_hbm,
    qn_hbm,
    qr_hbm,
    nl_hbm,
    nr_hbm,
    len_hbm,
    routes_hbm,
    gm_hbm,
    gf_hbm,
    go_hbm,
    ab_hbm,
    cl_hbm,
    cr_hbm,
    vup_hbm,
    wo_hbm,
    router_hbm,
    eg_hbm,
    eu_hbm,
    ed_hbm,
    sg_hbm,
    su_hbm,
    sd_hbm,
    out_ref,
    hidden,
    qn,
    qr,
    nl,
    nr,
    length_of,
    route_of,
    gm,
    gf,
    go,
    ab,
    keys,
    rope_keys,
    vraw,
    wo,
    router,
    egu,
    ed,
    sgu,
    sd,
    vup,
    wq,
    new_keys,
    scores,
    turned_weights,
    lat,
    xbuf,
    hbuf,
    cbuf,
    norm_rows,
    mix_rows,
    terms,
    back,
    local_sem,
    pair_send,
    pair_recv,
    far_send,
    far_recv,
    ready,
):
    seq_count, heads, nope = qn.shape
    rope = qr.shape[2]
    width = out_ref.shape[1]
    latent = nl.shape[1]
    rows = seq_count * heads
    chunks, _, unit, _ = hbuf.shape
    chunk_rows = ep_count * unit
    chunk_depth = unit * (latent + rope)
    bits = (ep_count - 1).bit_length()
    me_e = lax.axis_index("ep")
    me_t = lax.axis_index("tp")

    def device(e, t):
        return {"ep": e, "tp": t}

    sibling = device(me_e, 1 - me_t)
    far_first = list(range(ep_count - 1, 0, -1))
    barrier = pltpu.get_barrier_semaphore()

    def tell(semaphore, target):
        pl.semaphore_signal(
            semaphore, inc=1, device_id=target, device_id_type=pl.DeviceIdType.MESH
        )

    @pl.when(me_t == 1)
    def _():
        tell(barrier, sibling)

    sems = iter(range(local_sem.shape[0]))

    def fetch(source, target, sem=None):
        copy = pltpu.make_async_copy(source, target, local_sem.at[next(sems) if sem is None else sem])
        copy.start()
        return copy

    def all_of(region, sem):
        return pltpu.make_async_copy(region, region, local_sem.at[sem])

    len_copy = fetch(len_hbm, length_of)
    query_copies = [
        fetch(s, t) for s, t in ((qr_hbm, qr), (nl_hbm, nl), (nr_hbm, nr), (qn_hbm, qn))
    ]
    row_copies = [fetch(routes_hbm, route_of), fetch(hidden_hbm, hidden)]
    absorb_copy = fetch(ab_hbm, ab)
    value_copy = fetch(vup_hbm, vraw)
    rope_copy = fetch(cr_hbm, rope_keys)
    cache_copies = []
    for c in range(chunks):
        sem = next(sems)
        for i in range(unit):
            at = c * chunk_depth + i * latent
            fetch(cl_hbm.at[c * unit + i], keys.at[:, at : at + latent], sem)
        at = c * chunk_depth
        cache_copies.append(all_of(keys.at[:, at : at + unit * latent], sem))

    def to_sibling(index, source, target):
        return pltpu.make_async_remote_copy(
            src_ref=source,
            dst_ref=target,
            send_sem=pair_send.at[index],
            recv_sem=pair_recv.at[index],
            device_id=sibling,
            device_id_type=pl.DeviceIdType.MESH,
        )

    pair_copies = [
        to_sibling(index, source, target)
        for index, (source, target) in enumerate(
            (
                (wo_hbm, wo.at[me_t]),
                (eg_hbm, egu.at[me_t, 0]),
                (eu_hbm, egu.at[me_t, 1]),
                (ed_hbm, ed.at[me_t]),
            )
        )
    ]

    @pl.when(me_t == 0)
    def _():
        pl.semaphore_wait(barrier, 1)
        tell(ready.at[0], sibling)

    @pl.when(me_t == 1)
    def _():
        pl.semaphore_wait(ready.at[0], 1)
        for mask in far_first:
            tell(barrier, device(flip(me_e, mask, bits), me_t))

    for copy in pair_copies:
        copy.start()

    value_dim = vraw.shape[2]
    step = 256 // heads
    order_row = lax.broadcasted_iota(jnp.int32, (256, 256), 0)
    order_lane = lax.broadcasted_iota(jnp.int32, (256, 256), 1)
    order = jnp.where(
        order_lane == order_row % step * heads + order_row // step, 1.0, 0.0
    ).astype(jnp.bfloat16)

    half = rope // 2
    turn_row = lax.broadcasted_iota(jnp.int32, (seq_count, rope), 0)
    turn_lane = lax.broadcasted_iota(jnp.int32, (seq_count, rope), 1)
    inverse = jnp.zeros((seq_count, rope), jnp.float32)
    for i in range(half):
        inverse = jnp.where(turn_lane % half == i, rope_theta ** (-2.0 * i / rope), inverse)
    for copy in [len_copy, absorb_copy] + query_copies:
        copy.wait()
    position = jnp.zeros((seq_count, rope), jnp.float32)
    for s in range(seq_count):
        position = jnp.where(turn_row == s, length_of[s].astype(jnp.float32), position)
    angles = position * inverse
    cosine = jnp.cos(angles)
    sine = jnp.sin(angles) * jnp.where(turn_lane < half, -1.0, 1.0)

    def turned(values, cos_rows, sin_rows):
        swapped = jnp.concatenate([values[:, half:], values[:, :half]], axis=1)
        return values * cos_rows + swapped * sin_rows

    def per_head(table):
        return jnp.broadcast_to(table[:, None, :], (seq_count, heads, rope)).reshape(rows, rope)

    query_rows = qr[...].astype(jnp.float32).reshape(rows, rope)
    q_pe = turned(query_rows, per_head(cosine), per_head(sine))
    key_rows = turned(nr[...].astype(jnp.float32), cosine, sine)
    new_rows = normalize(nl[...].astype(jnp.float32)).astype(jnp.bfloat16).astype(jnp.float32)

    def places(s):
        base = s // unit * chunk_depth
        at = base + s % unit * latent
        rope_at = base + unit * latent + s % unit * rope
        return slice(at, at + latent), slice(rope_at, rope_at + rope)

    new_keys[...] = jnp.zeros_like(new_keys)
    for s in range(seq_count):
        new_keys[0:1, places(s)[0]] = new_rows[s : s + 1, :]
    for c in range(chunks):
        at = c * chunk_depth + unit * latent
        new_keys[0:1, at : at + unit * rope] = jnp.concatenate(
            [key_rows[s : s + 1, :] for s in range(c * unit, (c + 1) * unit)], axis=1
        )

    nope_rows = qn[...].astype(jnp.float32).reshape(rows, nope)
    row_head = lax.broadcasted_iota(jnp.int32, (rows, 2 * nope), 0) % heads
    pair_lane = lax.broadcasted_iota(jnp.int32, (rows, 2 * nope), 1) // nope
    doubled = jnp.concatenate([nope_rows, nope_rows], axis=1)
    spread_query = jnp.concatenate(
        [
            jnp.where(row_head == pair_lane + 2 * j, doubled, 0.0).astype(jnp.bfloat16)
            for j in range(heads // 2)
        ],
        axis=1,
    )
    q_lat = jnp.dot(spread_query, ab[...], preferred_element_type=jnp.float32)
    q_turned = q_lat.T
    lane_seq = lax.broadcasted_iota(jnp.int32, (latent, rows), 1) // heads
    rope_turned = jnp.concatenate([q_pe] * (128 // rope), axis=1).T[:rope]
    rope_seq = lax.broadcasted_iota(jnp.int32, (rope, rows), 1) // heads
    for s in range(seq_count):
        place, rope_place = places(s)
        wq[place, :] = jnp.where(lane_seq == s, q_turned, 0.0).astype(jnp.bfloat16)
        wq[rope_place, :] = jnp.where(rope_seq == s, rope_turned, 0.0).astype(jnp.bfloat16)

    for copy in row_copies + [value_copy, rope_copy]:
        copy.wait()
    for b in range(0, latent // step, 2):
        blocks = [
            vraw[i * step : (i + 1) * step].reshape(step * heads, value_dim) for i in (b, b + 1)
        ]
        ordered = jnp.dot(
            order, jnp.concatenate(blocks, axis=1), preferred_element_type=jnp.float32
        ).astype(jnp.bfloat16)
        for i in range(2):
            for h in range(heads):
                vup[(b + i) * step : (b + i + 1) * step, h * value_dim : (h + 1) * value_dim] = (
                    ordered[h * step : (h + 1) * step, i * value_dim : (i + 1) * value_dim]
                )

    mark_shape = (seq_count, xbuf.shape[3] - width)
    mark_row = lax.broadcasted_iota(jnp.int32, mark_shape, 0)
    mark_lane = lax.broadcasted_iota(jnp.int32, mark_shape, 1)
    marks = jnp.zeros(mark_shape, jnp.float32)
    for s in range(seq_count):
        for j in range(route_of.shape[0]):
            expert = route_of[j, me_t * seq_count + s]
            marks = jnp.where((mark_row == s) & (mark_lane == expert), 1.0, marks)
    own_rows = hidden[...].astype(jnp.float32)
    for c in range(chunks):
        part = slice(c * unit, (c + 1) * unit)
        xbuf[me_e, c, :, 0:width] = own_rows[part].astype(jnp.bfloat16)
        xbuf[me_e, c, :, width:] = marks[part].astype(jnp.bfloat16)

    context = keys.shape[0]
    lengths_row = jnp.zeros((1, rows), jnp.int32)
    lane_of = lax.broadcasted_iota(jnp.int32, (1, rows), 1) // heads
    for s in range(seq_count):
        lengths_row = jnp.where(lane_of == s, length_of[s], lengths_row)
    new_score = jnp.dot(
        new_keys[...].astype(jnp.bfloat16), wq[...], preferred_element_type=jnp.float32
    )[0:1]
    for c in range(chunks):
        at = c * chunk_depth + unit * latent
        keys[:, at : at + unit * rope] = rope_keys[c * unit * rope : (c + 1) * unit * rope].T

    block = 256
    key_index = lax.broadcasted_iota(jnp.int32, (block, rows), 0)
    power = score_scale * math.log2(math.e)

    def attend(c):
        deep = slice(c * chunk_depth, (c + 1) * chunk_depth)
        query = wq[deep, :]
        tops = jnp.full((8, rows), masked_score, jnp.float32)
        for k in range(0, context, block):
            found = jnp.dot(keys[k : k + block, deep], query, preferred_element_type=jnp.float32)
            found = jnp.where(key_index < lengths_row - k, found, masked_score)
            scores[k : k + block, :] = found
            tops = jnp.maximum(tops, jnp.max(found.reshape(block // 8, 8, rows), axis=0))
        row_max = jnp.maximum(jnp.max(tops, axis=0, keepdims=True), new_score)
        sums = jnp.zeros((8, rows), jnp.float32)
        for k in range(0, context, block):
            weights = jnp.exp2((scores[k : k + block, :] - row_max) * power)
            sums = sums + jnp.sum(weights.reshape(block // 8, 8, rows), axis=0)
            turned_weights[:, k : k + block] = weights.astype(jnp.bfloat16).T
        new_weight = jnp.exp2((new_score - row_max) * power)
        weight_total = jnp.sum(sums, axis=0, keepdims=True) + new_weight
        new_weight = new_weight.astype(jnp.bfloat16).astype(jnp.float32)
        side = jnp.concatenate(
            [weight_total, new_weight, jnp.zeros((6, rows), jnp.float32)], axis=0
        ).T
        for s in range(c * unit, (c + 1) * unit):
            part = slice(s * heads, (s + 1) * heads)
            weighted = jnp.dot(
                turned_weights[part, :], keys[:, places(s)[0]], preferred_element_type=jnp.float32
            )
            weighted = weighted + side[part, 1:2] * new_rows[s : s + 1, :]
            lat[part, :] = (weighted / side[part, 0:1]).astype(jnp.bfloat16)
        spread = jnp.dot(
            lat[c * unit * heads : (c + 1) * unit * heads, :],
            vup[...],
            preferred_element_type=jnp.float32,
        )
        own_heads = []
        head_row = lax.broadcasted_iota(jnp.int32, (unit, heads, value_dim), 1)
        for h in range(heads):
            piece = spread[:, h * value_dim : (h + 1) * value_dim].reshape(unit, heads, value_dim)
            own_heads.append(jnp.sum(jnp.where(head_row == h, piece, 0.0), axis=1))
        hbuf[c, me_e] = jnp.concatenate(own_heads, axis=1).astype(jnp.bfloat16)

    def remote(group, mask, source, target):
        return pltpu.make_async_remote_copy(
            src_ref=source,
            dst_ref=target,
            send_sem=far_send.at[group],
            recv_sem=far_recv.at[group],
            device_id=device(flip(me_e, mask, bits), me_t),
            device_id_type=pl.DeviceIdType.MESH,
        )

    def share(group, slot):
        for mask in far_first:
            remote(group, mask, slot, slot).start()

    peers = pl.ds(0, ep_count - 1)
    drains = []

    def gathered(group, region):
        whole = remote(group, 1, region, region)
        drains.append(whole)
        whole.wait_recv()

    def columns(c):
        flat_heads = hbuf[c].reshape(chunk_rows, hbuf.shape[3])
        cbuf[c, me_e] = jnp.concatenate(
            [
                jnp.dot(flat_heads, wo[t], preferred_element_type=jnp.float32)
                for t in range(wo.shape[0])
            ],
            axis=1,
        ).astype(jnp.bfloat16)
        share(2 + c, cbuf.at[c, me_e])

    def experts(c):
        mixed = jnp.concatenate([cbuf[c, o] for o in range(ep_count)], axis=1).astype(jnp.float32)
        stage = xbuf[:, c].reshape(chunk_rows, xbuf.shape[3])
        after_mix = (stage[:, :width].astype(jnp.float32) + gains[0] * normalize(mixed)).astype(
            jnp.bfloat16
        )
        mix_rows[c] = after_mix.reshape(ep_count, unit, width)
        ffn_in = (normalize(after_mix.astype(jnp.float32)) * gains[1]).astype(jnp.bfloat16)
        norm_rows[c] = ffn_in.reshape(ep_count, unit, width)
        affinity = jax.nn.sigmoid(
            lax.dot_general(
                ffn_in, router[...], (((1,), (1,)), ((), ())), preferred_element_type=jnp.float32
            )
        )
        hot = stage[:, width : width + affinity.shape[1]].astype(jnp.float32)
        chosen = affinity * hot
        lane = lax.broadcasted_iota(jnp.int32, chosen.shape, 1)
        whole = jnp.sum(chosen, axis=1, keepdims=True)
        outcome = jnp.zeros((chunk_rows, width), jnp.float32)
        for t in range(ed.shape[0]):
            mine = jnp.sum(jnp.where(lane == me_e * 2 + t, chosen, 0.0), axis=1, keepdims=True)
            mine = mine / whole * routed_scale
            expert_out = swiglu(ffn_in, egu[t, 0], egu[t, 1], ed[t])
            outcome = outcome + expert_out.astype(jnp.float32) * mine
        terms[c] = outcome.astype(jnp.bfloat16).reshape(ep_count, unit, width)
        for mask in far_first:
            remote(4 + c, mask, terms.at[c, flip(me_e, mask, bits)], back.at[c, me_e]).start()
        back[c, me_e] = terms[c, me_e]

    cross = ep_count // 2
    upper = me_e >= cross

    def open_plane():
        @pl.when(me_t == 1)
        def _():
            pl.semaphore_wait(barrier, ep_count - 1)
            tell(ready.at[1], sibling)

        @pl.when(me_t == 0)
        def _():
            pl.semaphore_wait(ready.at[1], 1)

    def spread_rows():
        remote(7, cross, xbuf.at[me_e], xbuf.at[me_e]).start()
        for mask in range(cross - 1, 0, -1):
            remote(6, mask, xbuf.at[me_e], xbuf.at[me_e]).start()

    @pl.when(upper)
    def _():
        open_plane()
        spread_rows()

    cache_copies[0].wait()
    attend(0)

    @pl.when(jnp.logical_not(upper))
    def _():
        open_plane()

    share(0, hbuf.at[0, me_e])

    @pl.when(jnp.logical_not(upper))
    def _():
        spread_rows()

    cache_copies[1].wait()
    wo_copy = fetch(wo_hbm, wo.at[me_t])
    gain_copies = [fetch(s, t) for s, t in ((gm_hbm, gm), (gf_hbm, gf), (go_hbm, go))]
    router_copy = fetch(router_hbm, router)
    sem = next(sems)
    fetch(eg_hbm, egu.at[me_t, 0], sem)
    fetch(eu_hbm, egu.at[me_t, 1], sem)
    expert_copies = [all_of(egu.at[me_t], sem), fetch(ed_hbm, ed.at[me_t])]
    sem = next(sems)
    fetch(sg_hbm, sgu.at[0], sem)
    fetch(su_hbm, sgu.at[1], sem)
    shared_copies = [all_of(sgu, sem), fetch(sd_hbm, sd)]
    attend(1)
    share(1, hbuf.at[1, me_e])

    wo_copy.wait()
    pair_copies[0].wait_recv()
    gathered(0, hbuf.at[0, peers])
    other = flip(me_e, cross, bits)
    crossed = remote(7, cross, xbuf.at[other], xbuf.at[other])
    crossed.wait_recv()
    for mask in range(cross - 1, 0, -1):
        remote(6, mask, xbuf.at[other], xbuf.at[other]).start()
    columns(0)
    gathered(1, hbuf.at[1, peers])
    columns(1)
    for copy in gain_copies + [router_copy] + expert_copies:
        copy.wait()
    for copy in pair_copies[1:]:
        copy.wait_recv()
    gains = [ref[...].astype(jnp.float32).reshape(1, width) for ref in (gm, gf, go)]
    gathered(2, cbuf.at[0, peers])
    gathered(6, xbuf.at[pl.ds(0, ep_count - 2)])
    experts(0)
    gathered(3, cbuf.at[1, peers])
    experts(1)
    for copy in shared_copies:
        copy.wait()
    own_in = jnp.concatenate(
        [norm_rows[c, me_e].astype(jnp.float32) for c in range(chunks)], axis=0
    ).astype(jnp.bfloat16)
    combined = swiglu(own_in, sgu[0], sgu[1], sd[...]).astype(jnp.float32)
    returned = []
    for c in range(chunks):
        gathered(4 + c, back.at[c, peers])
        returned.append(jnp.sum(back[c].astype(jnp.float32), axis=0))
    combined = combined + jnp.concatenate(returned, axis=0)
    own_mix = jnp.concatenate(
        [mix_rows[c, me_e].astype(jnp.float32) for c in range(chunks)], axis=0
    )
    out_ref[...] = (own_mix + gains[2] * normalize(combined)).astype(jnp.bfloat16)
    for copy in pair_copies + [crossed] + drains:
        copy.wait_send()


def local_fused(
    hidden_in,
    query_nope,
    query_rope,
    new_latent,
    new_rope,
    cache_latent,
    cache_rope,
    lengths,
    absorb_key,
    value_up,
    out_proj,
    gain_mix,
    gain_ffn_in,
    router,
    routes,
    expert_gate,
    expert_up,
    expert_down,
    shared_gate,
    shared_up,
    shared_down,
    gain_ffn_out,
):
    seq_count, width = hidden_in.shape
    heads, latent = query_nope.shape[1], cache_latent.shape[2]
    context, rope = cache_rope.shape[1:]
    ep_count = lax.axis_size("ep")
    bf = jnp.bfloat16
    score_scale = (query_nope.shape[-1] + query_rope.shape[-1]) ** (-0.5)
    dma = pltpu.SemaphoreType.DMA
    chunks = 2
    unit = seq_count // chunks
    total_rows = ep_count * seq_count
    rows = seq_count * heads
    depth = seq_count * (latent + rope)
    rope_rows = jnp.swapaxes(cache_rope, 1, 2).reshape(seq_count * rope, context)
    router_rows = jnp.swapaxes(router, 0, 1)
    absorb_rows = jnp.transpose(absorb_key, (1, 2, 0)).reshape(-1, latent)
    route_rows = jnp.swapaxes(routes, 0, 1)
    gate, up, down = expert_gate[0], expert_up[0], expert_down[0]
    operands = (
        hidden_in,
        query_nope,
        query_rope,
        new_latent,
        new_rope,
        lengths,
        route_rows,
        gain_mix,
        gain_ffn_in,
        gain_ffn_out,
        absorb_rows,
        cache_latent,
        rope_rows,
        value_up,
        out_proj,
        router_rows,
        gate,
        up,
        down,
        shared_gate,
        shared_up,
        shared_down,
    )

    def near(array, lead=()):
        return pltpu.VMEM(lead + array.shape, array.dtype)

    flops = 2 * total_rows * width * out_proj.shape[1]
    return pl.pallas_call(
        functools.partial(fused_kernel, ep_count, score_scale),
        out_shape=pltpu.VMEM((seq_count, width), bf),
        in_specs=[pl.BlockSpec(memory_space=pl.ANY)] * len(operands),
        out_specs=pl.BlockSpec(memory_space=pltpu.VMEM),
        scratch_shapes=[near(a) for a in operands[:5]]
        + [pltpu.SMEM(lengths.shape, jnp.int32), pltpu.SMEM(route_rows.shape, jnp.int32)]
        + [near(a) for a in operands[7:11]]
        + [
            pltpu.VMEM((context, depth), bf),
            near(rope_rows),
            near(value_up),
            near(out_proj, (2,)),
            near(router_rows),
            near(gate, (2, 2)),
            near(down, (2,)),
            near(shared_gate, (2,)),
            near(shared_down),
            pltpu.VMEM((latent, heads * value_up.shape[2]), bf),
            pltpu.VMEM((depth, rows), bf),
            pltpu.VMEM((8, depth), jnp.float32),
            pltpu.VMEM((context, rows), jnp.float32),
            pltpu.VMEM((rows, context), bf),
            pltpu.VMEM((rows, latent), bf),
            pltpu.VMEM((ep_count, chunks, unit, width + 128), bf),
            pltpu.VMEM((chunks, ep_count, unit, out_proj.shape[0]), bf),
            pltpu.VMEM((chunks, ep_count, ep_count * unit, 2 * out_proj.shape[1]), bf),
            pltpu.VMEM((chunks, ep_count, unit, width), bf),
            pltpu.VMEM((chunks, ep_count, unit, width), bf),
            pltpu.VMEM((chunks, ep_count, unit, width), bf),
            pltpu.VMEM((chunks, ep_count, unit, width), bf),
            dma((21,)),
            dma((4,)),
            dma((4,)),
            dma((8,)),
            dma((8,)),
            pltpu.SemaphoreType.REGULAR((2,)),
        ],
        compiler_params=pltpu.CompilerParams(
            collective_id=0, has_side_effects=True, vmem_limit_bytes=56 * 2**20
        ),
        cost_estimate=pl.CostEstimate(flops=flops, bytes_accessed=2**24, transcendentals=0),
        name="layer_step",
    )(*operands)


def local(*args):
    hidden_in, out_proj, router = args[0], args[10], args[13]
    device_count = lax.axis_size("ep") * lax.axis_size("tp")
    ep_count = lax.axis_size("ep")
    fits = (
        lax.axis_size("tp") == 2
        and ep_count & (ep_count - 1) == 0
        and ep_count >= 8
        and hidden_in.shape[0] == 8
        and args[1].shape[1] == 16
        and device_count * hidden_in.shape[0] <= 256
        and out_proj.shape[1] % 128 == 0
        and router.shape[1] == device_count
    )
    return local_fused(*args) if fits else local_wide(*args)


def solution(mesh):
    placed = (
        P(("grp", "ep", "tp"), None),
        P(("grp", "ep", "tp"), None, None),
        P(("grp", "ep", "tp"), None, None),
        P(("grp", "ep", "tp"), None),
        P(("grp", "ep", "tp"), None),
        P(("grp", "ep", "tp"), None, None),
        P(("grp", "ep", "tp"), None, None),
        P(("grp", "ep", "tp")),
        P(),
        P(),
        P(None, ("ep", "tp")),
        P(),
        P(),
        P(),
        P(("grp", "ep"), None),
        P(("ep", "tp"), None, None),
        P(("ep", "tp"), None, None),
        P(("ep", "tp"), None, None),
        P(),
        P(),
        P(),
        P(),
    )
    return jax.shard_map(
        local, mesh=mesh, in_specs=placed, out_specs=P(("grp", "ep", "tp"), None), check_vma=False
    )
```
